128 devices in a mesh: sp: 16 (over z, x), tp: 8 (over y, core).
Axes of the slice: x: 4, y: 4, z: 4, core: 2. Of those that a mesh axis runs over, the one named last changes fastest.
Arguments:
- query_small: bfloat16 [12288, 1024], P('sp', 'tp'), may hold values from -18 to 18
- key_small: bfloat16 [12288, 1024], P('sp', 'tp'), may hold values from -6 to 6
- value_small: bfloat16 [12288, 1024], P('sp', 'tp'), may hold values from -6 to 6
- offset_small: bfloat16 [16, 12288], P('tp', 'sp'), may hold values from -25 to 0
- query_large: bfloat16 [12288, 1024], P('sp', 'tp'), may hold values from -18 to 18
- key_large: bfloat16 [12288, 1024], P('sp', 'tp'), may hold values from -6 to 6
- value_large: bfloat16 [12288, 1024], P('sp', 'tp'), may hold values from -6 to 6
- offset_large: bfloat16 [8, 12288], P('tp', 'sp'), may hold values from -25 to 0
- out_small: bfloat16 [1024, 2048], P('tp'), may hold values from -0.125 to 0.125
- out_large: bfloat16 [1024, 2048], P('tp'), may hold values from -0.125 to 0.125
- residual: bfloat16 [12288, 2048], P(('sp', 'tp')), may hold values from -1.1953125 to 1.1953125
- norm_gain: bfloat16 [2048], replicated, may hold values from 0.099609375 to 1.8984375
- gate_weight: bfloat16 [2048, 5632], P('sp', 'tp'), may hold values from -0.125 to 0.125
- up_weight: bfloat16 [2048, 5632], P('sp', 'tp'), may hold values from -0.125 to 0.125
- down_weight: bfloat16 [5632, 2048], P('tp', 'sp'), may hold values from -0.078125 to 0.078125
Outputs:
- layer_out: bfloat16 [12288, 2048], P(('sp', 'tp'))
The draws below stay inside these ranges and needn't reach their ends.
All inputs are finite; a program needn't handle non-finite values.
Results may differ from the reference program's by a relative error of at most 0.023.
Values may be sent and summed in bfloat16 or wider, within the bound.
A program may use at most 128 MiB of HBM per device.

```python
import math
import jax
import jax.numpy as jnp
from jax import lax

D = 2048
HEADS_SMALL = 16
SMALL_DIM = 64
HEADS_LARGE = 8
LARGE_DIM = 128
FF = 5632
TOK_DEV = 768
SEQUENCE_LENGTH = 12288
N_TP = 8


def draw_offsets(key, head_count_list):
    random_keys = jax.random.split(key, 7)
    share = 0.5
    quick = jax.random.uniform(random_keys[0], (head_count_list,)) < share
    slow_base = math.log(0.35 / SEQUENCE_LENGTH) - 4.5 + jax.random.uniform(random_keys[1], (head_count_list,), minval=-0.5, maxval=0.5)
    quick_base = -8.4 + jax.random.uniform(random_keys[2], (head_count_list,), minval=-0.5, maxval=0.5)
    baseline_output = jnp.where(quick, quick_base, slow_base)
    position_shifts = jax.random.uniform(random_keys[3], (head_count_list, SEQUENCE_LENGTH // TOK_DEV), minval=-0.7, maxval=0.7)
    position_shifts = jnp.repeat(position_shifts, TOK_DEV, axis=1)
    approximate_output = jax.random.uniform(random_keys[4], (head_count_list, SEQUENCE_LENGTH), minval=-0.5, maxval=0.5)
    sample_spots = jax.random.randint(random_keys[5], (head_count_list, 3), 0, SEQUENCE_LENGTH)
    token_places = jnp.arange(SEQUENCE_LENGTH, dtype=jnp.int32)
    sample_draw = jnp.any(token_places[None, :, None] == sample_spots[:, None, :], axis=2)
    sample_draw_value = jax.random.uniform(random_keys[6], (head_count_list, SEQUENCE_LENGTH), minval=-1.5, maxval=-0.5)
    return jnp.where(sample_draw, sample_draw_value, baseline_output[:, None] + position_shifts + approximate_output).astype(jnp.float32)


def draw_offset_small(key, part):
    return draw_offsets(jax.random.fold_in(key, 11), HEADS_SMALL).astype(jnp.bfloat16)


def draw_offset_large(key, part):
    return draw_offsets(jax.random.fold_in(key, 23), HEADS_LARGE).astype(jnp.bfloat16)


def level_of(rng, extent, shards, least, largest):
    def one(dim, parts):
        steps = jax.random.uniform(jax.random.fold_in(jax.random.fold_in(rng, 6), dim), (parts,), jnp.float32, least / len(shards), largest / len(shards))
        return jnp.repeat(jnp.exp(steps), extent[dim] // parts).reshape((-1,) + (1,) * (len(extent) - dim - 1))

    factor_of = one(*shards[0])
    for cut in shards[1:]:
        factor_of = factor_of * one(*cut)
    return factor_of


def normal_values(rng, extent, width, limit, pieces=(), kind=jnp.bfloat16):
    result = width * jax.random.normal(rng, extent, jnp.float32)
    if pieces:
        result = result * level_of(rng, extent, pieces, -0.22, 0.18)
    return jnp.clip(result, -limit, limit).astype(kind)


def setup_inputs(seed: int = 0) -> dict:
    seeds = jax.random.split(jax.random.key(seed), 16)
    query_small = normal_values(seeds[0], (SEQUENCE_LENGTH, HEADS_SMALL * SMALL_DIM), 3.0, 18.0, ((0, 16), (1, 8)))
    key_small = normal_values(seeds[1], (SEQUENCE_LENGTH, HEADS_SMALL * SMALL_DIM), 1.0, 6.0, ((0, 16), (1, 8)))
    value_small = normal_values(seeds[2], (SEQUENCE_LENGTH, HEADS_SMALL * SMALL_DIM), 1.0, 6.0, ((0, 16), (1, 8)))
    offset_small = draw_offset_small(jax.random.fold_in(seeds[15], 71), 0)
    query_large = normal_values(seeds[4], (SEQUENCE_LENGTH, HEADS_LARGE * LARGE_DIM), 3.0, 18.0, ((0, 16), (1, 8)))
    key_large = normal_values(seeds[5], (SEQUENCE_LENGTH, HEADS_LARGE * LARGE_DIM), 1.0, 6.0, ((0, 16), (1, 8)))
    value_large = normal_values(seeds[6], (SEQUENCE_LENGTH, HEADS_LARGE * LARGE_DIM), 1.0, 6.0, ((0, 16), (1, 8)))
    offset_large = draw_offset_large(jax.random.fold_in(seeds[15], 71), 0)
    out_small = normal_values(seeds[8], (HEADS_SMALL * SMALL_DIM, D), (HEADS_SMALL * SMALL_DIM + HEADS_LARGE * LARGE_DIM) ** -0.5, 0.125, ((0, 8),))
    out_large = normal_values(seeds[9], (HEADS_LARGE * LARGE_DIM, D), (HEADS_SMALL * SMALL_DIM + HEADS_LARGE * LARGE_DIM) ** -0.5, 0.125, ((0, 8),))
    residual = normal_values(seeds[10], (SEQUENCE_LENGTH, D), 0.2, 1.1953125, ((0, 128),))
    norm_gain = jnp.clip(1.0 + 0.18 * jax.random.normal(seeds[11], (D,), jnp.float32), 0.099609375, 1.8984375).astype(jnp.bfloat16)
    gate_weight = normal_values(seeds[12], (D, FF), D ** -0.5, 0.125, ((0, 16), (1, 8)))
    up_weight = normal_values(seeds[13], (D, FF), D ** -0.5, 0.125, ((0, 16), (1, 8)))
    down_weight = normal_values(seeds[14], (FF, D), FF ** -0.5, 0.078125, ((0, 8), (1, 16)))
    return {"query_small": query_small, "key_small": key_small, "value_small": value_small, "offset_small": offset_small, "query_large": query_large, "key_large": key_large, "value_large": value_large, "offset_large": offset_large, "out_small": out_small, "out_large": out_large, "residual": residual, "norm_gain": norm_gain, "gate_weight": gate_weight, "up_weight": up_weight, "down_weight": down_weight}


def stick_group(query, random_keys, values, offset, head_depth):
    head_count_list = offset.shape[0]

    def per_head(args):
        head_query, head_keys, head_values, head_offset = args
        key_pos = jnp.arange(SEQUENCE_LENGTH, dtype=jnp.int32)

        def per_block(first_row):
            block_query = lax.dynamic_slice_in_dim(head_query, first_row, TOK_DEV, 0)
            logits = jnp.dot(block_query, head_keys.T, preferred_element_type=jnp.float32) * head_depth ** (-0.5)
            logits = logits + head_offset.astype(jnp.float32)[None, :]
            query_pos = first_row + jnp.arange(TOK_DEV, dtype=jnp.int32)
            before = key_pos[None, :] < query_pos[:, None]
            fail_all = jax.nn.log_sigmoid(-logits)
            log_pass = logits + fail_all
            log_fail = jnp.where(before, fail_all, 0.0)
            suffix = lax.cumsum(log_fail, axis=1, reverse=True) - log_fail
            weights = jnp.where(before, jnp.exp(log_pass + suffix), 0.0).astype(jnp.bfloat16)
            return jnp.dot(weights, head_values, preferred_element_type=jnp.float32).astype(jnp.bfloat16)
        starts = jnp.arange(SEQUENCE_LENGTH // TOK_DEV, dtype=jnp.int32) * TOK_DEV
        return lax.map(per_block, starts).reshape(SEQUENCE_LENGTH, head_depth)

    def split_heads(flat):
        return flat.reshape(SEQUENCE_LENGTH, head_count_list, head_depth).transpose(1, 0, 2)
    mixed = lax.map(per_head, (split_heads(query), split_heads(random_keys), split_heads(values), offset))
    return mixed.transpose(1, 0, 2).reshape(SEQUENCE_LENGTH, head_count_list * head_depth)

def rounded(value):
    return lax.optimization_barrier(value.astype(jnp.bfloat16)).astype(jnp.float32)

def reference(query_small, key_small, value_small, offset_small, query_large, key_large, value_large, offset_large, out_small, out_large, residual, norm_gain, gate_weight, up_weight, down_weight):
    mixed_small = stick_group(query_small, key_small, value_small, offset_small, SMALL_DIM)
    mixed_large = stick_group(query_large, key_large, value_large, offset_large, LARGE_DIM)
    small_run = HEADS_SMALL * SMALL_DIM // N_TP
    large_run = HEADS_LARGE * LARGE_DIM // N_TP
    total = jnp.zeros((SEQUENCE_LENGTH, D), jnp.float32)
    for group in range(N_TP):
        part = jnp.dot(mixed_small[:, group * small_run:(group + 1) * small_run], out_small[group * small_run:(group + 1) * small_run], preferred_element_type=jnp.float32)
        part = part + jnp.dot(mixed_large[:, group * large_run:(group + 1) * large_run], out_large[group * large_run:(group + 1) * large_run], preferred_element_type=jnp.float32)
        total = total + rounded(part)
    stream = residual.astype(jnp.float32) + rounded(total)
    scale = lax.rsqrt(lax.optimization_barrier(jnp.mean(stream * stream, axis=-1, keepdims=True)) + 1e-06)
    normed = (stream * scale * norm_gain.astype(jnp.float32)).astype(jnp.bfloat16)
    gate = jnp.dot(normed, gate_weight, preferred_element_type=jnp.float32)
    upper = jnp.dot(normed, up_weight, preferred_element_type=jnp.float32)
    hidden = (jax.nn.silu(gate) * upper).astype(jnp.bfloat16)
    hidden_run = FF // N_TP
    summed = jnp.zeros((SEQUENCE_LENGTH, D), jnp.float32)
    for group in range(N_TP):
        part = jnp.dot(hidden[:, group * hidden_run:(group + 1) * hidden_run], down_weight[group * hidden_run:(group + 1) * hidden_run], preferred_element_type=jnp.float32)
        summed = summed + rounded(part)
    return (stream + rounded(summed)).astype(jnp.bfloat16)
```

```python
import functools
import math

import jax
import jax.numpy as jnp
import numpy as np
from jax import lax
from jax.experimental import pallas as pl
from jax.experimental.pallas import tpu as pltpu
from jax.sharding import PartitionSpec as P

SMALL_DIM = 64
LARGE_DIM = 128
BLOCK = 768
STRIPES = 8
STRIPE = BLOCK // STRIPES
TILE = 256
LOG2E = math.log2(math.e)
MESH = pl.DeviceIdType.MESH
VMEM_LIMIT = 60 * 1024 * 1024


def vmem():
    return pl.BlockSpec(memory_space=pltpu.VMEM)


def sp_coords():
    index = lax.axis_index("sp")
    return index // 4, index % 4


def z_neighbours():
    z, x = sp_coords()
    return {"sp": ((z + 1) % 4) * 4 + x}, {"sp": ((z + 3) % 4) * 4 + x}


def x_neighbours():
    z, x = sp_coords()
    return {"sp": z * 4 + (x + 1) % 4}, {"sp": z * 4 + (x + 3) % 4}


def y_neighbours():
    t = lax.axis_index("tp")
    return {"tp": (t + 2) % 8}, {"tp": (t + 6) % 8}


def sibling():
    t = lax.axis_index("tp")
    return {"tp": t + 1 - 2 * (t % 2)}


def greet(devices):
    barrier = pltpu.get_barrier_semaphore()
    for device in devices:
        pl.semaphore_signal(barrier, inc=1, device_id=device, device_id_type=MESH)
    pl.semaphore_wait(barrier, len(devices))


class Copies:
    def __init__(self, send_sems, recv_sems):
        self.send_sems, self.recv_sems, self.used, self.all = send_sems, recv_sems, 0, []

    def make(self, src, dst, device):
        k = self.used
        self.used += 1
        copy = pltpu.make_async_remote_copy(
            src_ref=src,
            dst_ref=dst,
            send_sem=self.send_sems.at[k],
            recv_sem=self.recv_sems.at[k],
            device_id=device,
            device_id_type=MESH,
        )
        self.all.append(copy)
        return copy

    def drain_sends(self):
        for copy in self.all:
            copy.wait_send()


def comm_call(kernel, outs, scratch, copies, collective_id, name, args):
    return pl.pallas_call(
        kernel,
        out_shape=outs,
        in_specs=[vmem()] * len(args),
        out_specs=jax.tree.map(lambda _: vmem(), outs),
        scratch_shapes=[
            *scratch,
            pltpu.SemaphoreType.DMA((copies,)),
            pltpu.SemaphoreType.DMA((copies,)),
        ],
        compiler_params=pltpu.CompilerParams(
            collective_id=collective_id, has_side_effects=True, vmem_limit_bytes=VMEM_LIMIT
        ),
        name=name,
    )(*args)


def ring_gather(copies, jobs):
    begun = []
    for own, whole, me, right, left, rows in jobs:
        to_right = copies.make(own, whole.at[me], right)
        to_left = copies.make(own, whole.at[me], left)
        to_right.start()
        to_left.start()
        begun.append((to_right, to_left))
    for own, whole, me, right, left, rows in jobs:
        whole[me] = own[...]
    later = []
    for (own, whole, me, right, left, rows), (to_right, to_left) in zip(jobs, begun):
        half = rows // 2
        before, after = (me + 3) % 4, (me + 1) % 4
        to_right.wait_recv()
        first = whole.at[before, pl.ds(0, half)]
        on_right = copies.make(first, first, right)
        on_right.start()
        to_left.wait_recv()
        second = whole.at[after, pl.ds(half, half)]
        on_left = copies.make(second, second, left)
        on_left.start()
        later.append((on_right, on_left))
    for on_right, on_left in later:
        on_right.wait_recv()
        on_left.wait_recv()
    copies.drain_sends()


def gather_kernel(q, k, v, off, q_all, k_all, v_all, off_all, send_sems, recv_sems):
    z, x = sp_coords()
    z_right, z_left = z_neighbours()
    x_right, x_left = x_neighbours()
    greet((z_right, z_left, x_right, x_left))
    ring_gather(
        Copies(send_sems, recv_sems),
        (
            (k, k_all, z, z_right, z_left, BLOCK),
            (q, q_all, x, x_right, x_left, 256),
            (v, v_all, z, z_right, z_left, 256),
            (off, off_all, z, z_right, z_left, 32),
        ),
    )


def totals_kernel(tot, tot_all, send_sems, recv_sems):
    _, x = sp_coords()
    right, left = x_neighbours()
    greet((right, left))
    ring_gather(Copies(send_sems, recv_sems), ((tot, tot_all, x, right, left, 16),))


def ring_sum(copies, parts, relay, arrived, me, right, left, rows, out):
    half = rows // 2
    top, low = pl.ds(0, half), pl.ds(half, half)
    far, after, before = (me + 2) % 4, (me + 1) % 4, (me + 3) % 4
    a = copies.make(parts.at[far, top], relay.at[0], right)
    b = copies.make(parts.at[far, low], relay.at[1], left)
    a.start()
    b.start()
    a.wait_recv()
    parts[after, top] = (
        parts[after, top].astype(jnp.float32) + relay[0].astype(jnp.float32)
    ).astype(jnp.bfloat16)
    c = copies.make(parts.at[after], arrived.at[0], right)
    c.start()
    b.wait_recv()
    parts[before, low] = (
        parts[before, low].astype(jnp.float32) + relay[1].astype(jnp.float32)
    ).astype(jnp.bfloat16)
    d = copies.make(parts.at[before], arrived.at[1], left)
    d.start()
    c.wait_recv()
    d.wait_recv()
    out[...] = (
        parts[me].astype(jnp.float32)
        + arrived[0].astype(jnp.float32)
        + arrived[1].astype(jnp.float32)
    ).astype(out.dtype)
    copies.drain_sends()


def x_sum_kernel(parts_in, out, parts, relay, arrived, send_sems, recv_sems):
    _, x = sp_coords()
    right, left = x_neighbours()
    greet((right, left))
    parts[...] = parts_in[...]
    ring_sum(Copies(send_sems, recv_sems), parts, relay, arrived, x, right, left, 256, out)


def tp_sum_kernel(terms, out, other, parts, relay, arrived, send_sems, recv_sems):
    t = lax.axis_index("tp")
    y, core = t // 2, t % 2
    right, left = y_neighbours()
    mate = sibling()
    greet((right, left, mate))
    copies = Copies(send_sems, recv_sems)
    order = [(y + step) % 4 for step in (2, 1, 3, 0)]
    given = []
    for place in order:
        copy = copies.make(terms.at[place, 1 - core], other.at[place], mate)
        copy.start()
        given.append(copy)
    for place, copy in zip(order, given):
        copy.wait_recv()
        parts[place] = (
            terms[place, core].astype(jnp.float32) + other[place].astype(jnp.float32)
        ).astype(jnp.bfloat16)
    ring_sum(copies, parts, relay, arrived, y, right, left, 96, out)


def tp_gather_kernel(own, whole, send_sems, recv_sems):
    t = lax.axis_index("tp")
    y, core = t // 2, t % 2
    right, left = y_neighbours()
    mate = sibling()
    greet((right, left, mate))
    copies = Copies(send_sems, recv_sems)
    before, after, far = (y + 3) % 4, (y + 1) % 4, (y + 2) % 4
    top, low = pl.ds(0, 48), pl.ds(48, 48)
    mine = whole.at[y, core]
    to_right = copies.make(own, mine, right)
    to_left = copies.make(own, mine, left)
    across = copies.make(own, mine, mate)
    to_right.start()
    to_left.start()
    across.start()
    whole[y, core] = own[...]
    to_right.wait_recv()
    first = whole.at[before, core, top]
    on_right = copies.make(first, first, right)
    on_right.start()
    to_left.wait_recv()
    second = whole.at[after, core, low]
    on_left = copies.make(second, second, left)
    on_left.start()
    over = [across]
    for block in (whole.at[before, core], whole.at[after, core]):
        copy = copies.make(block, block, mate)
        copy.start()
        over.append(copy)
    on_right.wait_recv()
    block = whole.at[far, core, top]
    copy = copies.make(block, block, mate)
    copy.start()
    over.append(copy)
    on_left.wait_recv()
    block = whole.at[far, core, low]
    copy = copies.make(block, block, mate)
    copy.start()
    over.append(copy)
    for copy in over:
        copy.wait_recv()
    copies.drain_sends()


def selector(head):
    rows = lax.broadcasted_iota(jnp.int32, (128, TILE), 0)
    pieces, rest = [], LOG2E
    for _ in range(3):
        piece = float(np.asarray(rest, dtype=jnp.bfloat16.dtype).astype(np.float64))
        pieces.append(piece)
        rest -= piece
    value = jnp.zeros((128, TILE), jnp.float32)
    for n, piece in enumerate(pieces):
        value = jnp.where(rows == 3 * head + n, piece, value)
    return value.astype(jnp.bfloat16)


HEADS = ((0, 0, 0, 64), (1, 0, 64, 64), (2, 128, 128, 128))


def attend_kernel(q_ref, k_ref, ext_ref, v_ref, o_ref, tot_ref, work_ref, rhs_ref):
    z, x = sp_coords()
    kb = pl.program_id(0)

    @pl.when(kb == 0)
    def _():
        tot_ref[...] = jnp.zeros_like(tot_ref)
        for head, key_column, row, rows in HEADS:
            rhs_ref[head, 128:256, :] = selector(head)
            if rows == 64:
                rhs_ref[head, 64 - row : 128 - row, :] = jnp.zeros((64, TILE), jnp.bfloat16)

    def tile(i, carry):
        place = i // 3
        first = pl.multiple_of((i % 3) * TILE, TILE)
        column = pl.multiple_of(i * TILE, TILE)
        columns = pl.ds(column, TILE)

        def run(masked):
            for head, key_column, row, rows in HEADS:
                inner = row if rows == 64 else 0
                rhs_ref[head, inner : inner + rows, :] = q_ref[place, row : row + rows, pl.ds(first, TILE)]
                rhs = rhs_ref[head]
                sums = jnp.zeros((8, TILE), jnp.float32)
                chunk = 128
                for c in reversed(range(BLOCK // chunk)):
                    span = slice(c * chunk, (c + 1) * chunk)
                    lhs = jnp.concatenate(
                        [k_ref[0, span, key_column : key_column + 128], ext_ref[0, span, :]], axis=1
                    )
                    logit = jnp.dot(lhs, rhs, preferred_element_type=jnp.float32)
                    loss = jnp.maximum(
                        logit, jnp.log2(1.0 + jnp.exp2(jnp.minimum(logit, 100.0)))
                    )
                    if masked:
                        at = lax.broadcasted_iota(jnp.int32, (chunk, TILE), 0) + c * chunk
                        key_pos = (at % 8) * STRIPE + at // 8
                        query_pos = lax.broadcasted_iota(jnp.int32, (chunk, TILE), 1) + first
                        live = key_pos < query_pos
                        loss = jnp.where(live, loss, 0.0)
                        logit = jnp.where(live, logit, -1e30)
                    for j in reversed(range(chunk // 8)):
                        eight = slice(j * 8, (j + 1) * 8)
                        sums = sums + loss[eight]
                        work_ref[c * chunk + j * 8 : c * chunk + (j + 1) * 8, :] = logit[eight] - sums
                later = [jnp.zeros((1, TILE), jnp.float32)]
                for r in range(7, 0, -1):
                    later.append(later[-1] + sums[r : r + 1])
                tot_ref[pl.ds(kb * 4 + head, 1), columns] = later[-1] + sums[0:1]
                behind = jnp.concatenate(later[::-1], axis=0)
                total = jnp.zeros((rows, TILE), jnp.float32)
                for c in range(BLOCK // 256):
                    span = slice(c * 256, (c + 1) * 256)
                    power = work_ref[span, :].reshape(32, 8, TILE) - behind[None]
                    weight = jnp.exp2(power).reshape(256, TILE).astype(jnp.bfloat16)
                    total = total + jnp.dot(
                        v_ref[0, row : row + rows, span], weight, preferred_element_type=jnp.float32
                    )
                o_ref[0, row : row + rows, columns] = total.astype(jnp.bfloat16)

        whole = jnp.logical_or(kb < z, jnp.logical_and(kb == z, place > x))
        partly = jnp.logical_and(kb == z, place == x)

        @pl.when(whole)
        def _():
            run(False)

        @pl.when(partly)
        def _():
            run(True)

        @pl.when(jnp.logical_not(jnp.logical_or(whole, partly)))
        def _():
            o_ref[0, :, columns] = jnp.zeros((256, TILE), jnp.bfloat16)

        return carry

    lax.fori_loop(0, 12, tile, 0)


def attend(q_all, k_all, ext, v_all):
    units = 12 * 8
    return pl.pallas_call(
        attend_kernel,
        grid=(4,),
        in_specs=[
            pl.BlockSpec((4, 256, BLOCK), lambda kb: (0, 0, 0)),
            pl.BlockSpec((1, BLOCK, 256), lambda kb: (kb, 0, 0)),
            pl.BlockSpec((1, BLOCK, 128), lambda kb: (kb, 0, 0)),
            pl.BlockSpec((1, 256, BLOCK), lambda kb: (kb, 0, 0)),
        ],
        out_specs=[
            pl.BlockSpec((1, 256, 4 * BLOCK), lambda kb: (kb, 0, 0)),
            pl.BlockSpec((16, 4 * BLOCK), lambda kb: (0, 0)),
        ],
        out_shape=[
            jax.ShapeDtypeStruct((4, 256, 4 * BLOCK), jnp.bfloat16),
            jax.ShapeDtypeStruct((16, 4 * BLOCK), jnp.float32),
        ],
        scratch_shapes=[
            pltpu.VMEM((BLOCK, TILE), jnp.float32),
            pltpu.VMEM((3, 256, TILE), jnp.bfloat16),
        ],
        compiler_params=pltpu.CompilerParams(
            dimension_semantics=("arbitrary",), vmem_limit_bytes=VMEM_LIMIT
        ),
        cost_estimate=pl.CostEstimate(
            flops=units * 768 * 768 * 1024, bytes_accessed=12_000_000, transcendentals=units * 768 * 768 * 9
        ),
        name="attend",
    )(q_all, k_all, ext, v_all)


def combine_kernel(o_ref, tot_ref, out_ref):
    _, x = sp_coords()
    nearer = jnp.zeros((4, TILE), jnp.float32)
    total = [None] * 3
    for kb in reversed(range(4)):
        rows = slice(kb * 4, kb * 4 + 4)
        here = jnp.zeros((4, TILE), jnp.float32)
        block = jnp.zeros((4, TILE), jnp.float32)
        for other in range(4):
            term = tot_ref[other, rows, :]
            block = block + term
            here = here + jnp.where(other > x, term, 0.0)
        factor = jnp.exp2(-(nearer + here))
        nearer = nearer + block
        for head, _, row, size in HEADS:
            term = o_ref[kb, row : row + size, :].astype(jnp.float32) * factor[head : head + 1]
            total[head] = term if total[head] is None else total[head] + term
    for head, _, row, size in HEADS:
        out_ref[0, row : row + size, :] = total[head].astype(jnp.bfloat16)


def combine(outs, totals):
    return pl.pallas_call(
        combine_kernel,
        grid=(12,),
        in_specs=[
            pl.BlockSpec((4, 256, TILE), lambda i: (0, 0, i)),
            pl.BlockSpec((4, 16, TILE), lambda i: (0, 0, i)),
        ],
        out_specs=pl.BlockSpec((1, 256, TILE), lambda i: (i // 3, 0, i % 3)),
        out_shape=jax.ShapeDtypeStruct((4, 256, BLOCK), jnp.bfloat16),
        compiler_params=pltpu.CompilerParams(dimension_semantics=("arbitrary",)),
        cost_estimate=pl.CostEstimate(
            flops=4 * 256 * 3072 * 2, bytes_accessed=9_000_000, transcendentals=50_000
        ),
        name="combine",
    )(outs, totals)


def tp_sum(terms, collective_id, name):
    shape = (96, terms.shape[-1])
    return comm_call(
        tp_sum_kernel,
        jax.ShapeDtypeStruct(shape, jnp.float32),
        [
            pltpu.VMEM((4, *shape), jnp.bfloat16),
            pltpu.VMEM((4, *shape), jnp.bfloat16),
            pltpu.VMEM((2, 48, shape[1]), jnp.bfloat16),
            pltpu.VMEM((2, *shape), jnp.bfloat16),
        ],
        8,
        collective_id,
        name,
        (terms.reshape(4, 2, *shape),),
    )


def rounded(value):
    return lax.optimization_barrier(value.astype(jnp.bfloat16)).astype(jnp.float32)


def rms_norm(stream, gain):
    scale = lax.rsqrt(jnp.mean(stream * stream, axis=-1, keepdims=True) + 1e-06)
    return (stream * scale * gain.astype(jnp.float32)).astype(jnp.bfloat16)


def striped(value):
    return value.reshape(STRIPES, STRIPE, -1).swapaxes(0, 1).reshape(BLOCK, -1)


def on_device(
    query_small, key_small, value_small, offset_small, query_large, key_large, value_large, offset_large,
    out_small, out_large, residual, norm_gain, gate_weight, up_weight, down_weight,
):
    f32, bf16 = jnp.float32, jnp.bfloat16
    scales = np.concatenate(
        [np.full(128, LOG2E * SMALL_DIM**-0.5), np.full(128, LOG2E * LARGE_DIM**-0.5)]
    ).astype(np.float32)
    query = jnp.concatenate([query_small, query_large], axis=1).astype(f32) * scales
    query = query.astype(bf16).T
    key = striped(jnp.concatenate([key_small, key_large], axis=1))
    value = striped(jnp.concatenate([value_small, value_large], axis=1)).T
    offsets = jnp.concatenate([offset_small, offset_large], axis=0)
    offsets = offsets.reshape(3, STRIPES, STRIPE).swapaxes(1, 2).reshape(3, BLOCK)
    offsets = jnp.pad(offsets, ((0, 29), (0, 0)))
    gathered = comm_call(
        gather_kernel,
        (
            jax.ShapeDtypeStruct((4, 256, BLOCK), bf16),
            jax.ShapeDtypeStruct((4, BLOCK, 256), bf16),
            jax.ShapeDtypeStruct((4, 256, BLOCK), bf16),
            jax.ShapeDtypeStruct((4, 32, BLOCK), bf16),
        ),
        [],
        16,
        0,
        "gather_qkv",
        (query, key, value, offsets),
    )
    gate_weight, up_weight, down_weight, *gathered = lax.optimization_barrier(
        (gate_weight, up_weight, down_weight, *gathered)
    )
    q_all, k_all, v_all, off_all = gathered
    weights = jnp.concatenate([gate_weight, up_weight, down_weight.T], axis=1)
    weights = lax.all_gather(weights, "sp", axis=0, tiled=True)
    width = gate_weight.shape[1]
    spread = np.zeros((32, 128), np.float32)
    for head in range(3):
        spread[head, 3 * head : 3 * head + 3] = 1
    ext = jnp.einsum(
        "bhs,hc->bsc", off_all, jnp.asarray(spread, bf16), preferred_element_type=f32
    ).astype(bf16)
    outs, totals = attend(q_all, k_all, ext, v_all)
    totals = comm_call(
        totals_kernel, jax.ShapeDtypeStruct((4, 16, 4 * BLOCK), f32), [], 4, 1, "gather_totals", (totals,)
    )
    parts = combine(outs, totals)
    mixed = comm_call(
        x_sum_kernel,
        jax.ShapeDtypeStruct((256, BLOCK), bf16),
        [
            pltpu.VMEM((4, 256, BLOCK), bf16),
            pltpu.VMEM((2, 128, BLOCK), bf16),
            pltpu.VMEM((2, 256, BLOCK), bf16),
        ],
        4,
        2,
        "sum_x",
        (parts,),
    )
    out_weight = jnp.concatenate([out_small, out_large], axis=0)
    part = lax.dot_general(mixed, out_weight, (((0,), (0,)), ((), ())), preferred_element_type=f32)
    attended = tp_sum(part.astype(bf16), 3, "sum_tp_mixed")
    stream = residual.astype(f32) + rounded(attended)
    normed = rms_norm(stream, norm_gain)
    rows = comm_call(
        tp_gather_kernel, jax.ShapeDtypeStruct((4, 2, 96, 2048), bf16), [], 9, 4, "gather_tp", (normed,)
    ).reshape(BLOCK, 2048)
    gate = jnp.dot(rows, weights[:, :width], preferred_element_type=f32)
    upper = jnp.dot(rows, weights[:, width : 2 * width], preferred_element_type=f32)
    hidden = (jax.nn.silu(gate) * upper).astype(bf16)
    down = lax.dot_general(
        hidden, weights[:, 2 * width :], (((1,), (1,)), ((), ())), preferred_element_type=f32
    )
    summed = tp_sum(down.astype(bf16), 5, "sum_tp_down")
    return (stream + rounded(summed)).astype(bf16)


def solution(mesh):
    return jax.shard_map(
        on_device,
        mesh=mesh,
        in_specs=(
            P("sp", "tp"), P("sp", "tp"), P("sp", "tp"), P("tp", "sp"),
            P("sp", "tp"), P("sp", "tp"), P("sp", "tp"), P("tp", "sp"),
            P("tp", None), P("tp", None), P(("sp", "tp"), None), P(),
            P("sp", "tp"), P("sp", "tp"), P("tp", "sp"),
        ),
        out_specs=P(("sp", "tp"), None),
        check_vma=False,
    )
```

```python
import functools
import math

import jax
import jax.numpy as jnp
import numpy as np
from jax import lax
from jax.experimental import pallas as pl
from jax.experimental.pallas import tpu as pltpu
from jax.sharding import PartitionSpec as P

SMALL_DIM = 64
LARGE_DIM = 128
BLOCK = 768
STRIPES = 8
STRIPE = BLOCK // STRIPES
TILE = 256
HALF = BLOCK // 2
LOG2E = math.log2(math.e)
MESH = pl.DeviceIdType.MESH
VMEM_LIMIT = 60 * 1024 * 1024


def vmem():
    return pl.BlockSpec(memory_space=pltpu.VMEM)


def sp_coords():
    index = lax.axis_index("sp")
    return index // 4, index % 4


def z_neighbours():
    z, x = sp_coords()
    return {"sp": ((z + 1) % 4) * 4 + x}, {"sp": ((z + 3) % 4) * 4 + x}


def x_neighbours():
    z, x = sp_coords()
    return {"sp": z * 4 + (x + 1) % 4}, {"sp": z * 4 + (x + 3) % 4}


def mirror():
    z, x = sp_coords()
    return {"sp": (3 - z) * 4 + x}


def y_neighbours():
    t = lax.axis_index("tp")
    return {"tp": (t + 2) % 8}, {"tp": (t + 6) % 8}


def sibling():
    t = lax.axis_index("tp")
    return {"tp": t + 1 - 2 * (t % 2)}


def greet(devices):
    barrier = pltpu.get_barrier_semaphore()
    for device in devices:
        pl.semaphore_signal(barrier, inc=1, device_id=device, device_id_type=MESH)
    pl.semaphore_wait(barrier, len(devices))


class Copies:
    def __init__(self, send_sems, recv_sems):
        self.send_sems, self.recv_sems, self.used, self.all = send_sems, recv_sems, 0, []

    def make(self, src, dst, device):
        k = self.used
        self.used += 1
        copy = pltpu.make_async_remote_copy(
            src_ref=src,
            dst_ref=dst,
            send_sem=self.send_sems.at[k],
            recv_sem=self.recv_sems.at[k],
            device_id=device,
            device_id_type=MESH,
        )
        self.all.append(copy)
        return copy

    def drain_sends(self):
        for copy in self.all:
            copy.wait_send()


def comm_call(kernel, outs, scratch, copies, collective_id, name, args):
    return pl.pallas_call(
        kernel,
        out_shape=outs,
        in_specs=[vmem()] * len(args),
        out_specs=jax.tree.map(lambda _: vmem(), outs),
        scratch_shapes=[
            *scratch,
            pltpu.SemaphoreType.DMA((copies,)),
            pltpu.SemaphoreType.DMA((copies,)),
        ],
        compiler_params=pltpu.CompilerParams(
            collective_id=collective_id, has_side_effects=True, vmem_limit_bytes=VMEM_LIMIT
        ),
        name=name,
    )(*args)


def ring_gather(copies, jobs):
    begun = []
    for own, whole, me, right, left, rows, wait in jobs:
        if wait is not None:
            wait()
        half = rows // 2
        top, low = pl.ds(0, half), pl.ds(half, half)
        sent = (
            copies.make(own.at[top], whole.at[me, top], right),
            copies.make(own.at[low], whole.at[me, low], left),
            copies.make(own.at[low], whole.at[me, low], right),
            copies.make(own.at[top], whole.at[me, top], left),
        )
        for copy in sent:
            copy.start()
        whole[me] = own[...]
        begun.append(sent)
    later = []
    for (own, whole, me, right, left, rows, wait), sent in zip(jobs, begun):
        half = rows // 2
        before, after = (me + 3) % 4, (me + 1) % 4
        sent[0].wait_recv()
        first = whole.at[before, pl.ds(0, half)]
        on_right = copies.make(first, first, right)
        on_right.start()
        sent[1].wait_recv()
        second = whole.at[after, pl.ds(half, half)]
        on_left = copies.make(second, second, left)
        on_left.start()
        later += [sent[2], sent[3], on_right, on_left]
    for copy in later:
        copy.wait_recv()
    copies.drain_sends()


def gather_kernel(
    q_own, q_give, k, v, off, qa_all, qb_all, k_all, v_all, off_all, q_got, send_sems, recv_sems
):
    z, x = sp_coords()
    z_right, z_left = z_neighbours()
    x_right, x_left = x_neighbours()
    greet((z_right, z_left, x_right, x_left))
    copies = Copies(send_sems, recv_sems)
    swap = copies.make(q_give, q_got, mirror())
    swap.start()
    ring_gather(
        copies,
        (
            (k, k_all, z, z_right, z_left, BLOCK, None),
            (v, v_all, z, z_right, z_left, 256, None),
            (off, off_all, z, z_right, z_left, 32, None),
            (q_own, qa_all, x, x_right, x_left, 256, None),
            (q_got, qb_all, x, x_right, x_left, 256, swap.wait_recv),
        ),
    )


def totals_kernel(tot, tot_all, send_sems, recv_sems):
    _, x = sp_coords()
    right, left = x_neighbours()
    greet((right, left))
    ring_gather(Copies(send_sems, recv_sems), ((tot, tot_all, x, right, left, 16, None),))


def plus(a, b):
    return (a.astype(jnp.float32) + b.astype(jnp.float32)).astype(jnp.bfloat16)


class RingSum:
    def __init__(self, copies, parts, relay, arrived, me, right, left, rows):
        half = rows // 2
        self.copies, self.parts, self.relay, self.arrived = copies, parts, relay, arrived
        self.me, self.right, self.left = me, right, left
        self.top, self.low = pl.ds(0, half), pl.ds(half, half)
        self.far, self.after, self.before = (me + 2) % 4, (me + 1) % 4, (me + 3) % 4
        self.waits = []

    def send(self, src, dst, device):
        copy = self.copies.make(src, dst, device)
        copy.start()
        return copy

    def send_far(self):
        self.a = self.send(self.parts.at[self.far, self.top], self.relay.at[0], self.right)
        self.b = self.send(self.parts.at[self.far, self.low], self.relay.at[1], self.left)

    def send_after(self):
        self.waits.append(
            self.send(self.parts.at[self.after, self.low], self.arrived.at[0, self.low], self.right)
        )

    def send_before(self):
        self.waits.append(
            self.send(self.parts.at[self.before, self.top], self.arrived.at[1, self.top], self.left)
        )

    def pass_on(self):
        self.a.wait_recv()
        self.parts[self.after, self.top] = plus(self.parts[self.after, self.top], self.relay[0])
        self.waits.append(
            self.send(self.parts.at[self.after, self.top], self.arrived.at[0, self.top], self.right)
        )
        self.b.wait_recv()
        self.parts[self.before, self.low] = plus(self.parts[self.before, self.low], self.relay[1])
        self.waits.append(
            self.send(self.parts.at[self.before, self.low], self.arrived.at[1, self.low], self.left)
        )

    def finish(self, own):
        for copy in self.waits:
            copy.wait_recv()
        return own + self.arrived[0].astype(jnp.float32) + self.arrived[1].astype(jnp.float32)


def x_sum_kernel(
    parts_a, parts_b, out, pa, pb, relay_a, relay_b, arrived_a, arrived_b, give, got, send_sems, recv_sems
):
    z, x = sp_coords()
    right, left = x_neighbours()
    greet((right, left, mirror()))
    copies = Copies(send_sems, recv_sems)
    rings = []
    for source, parts, relay, arrived in (
        (parts_b, pb, relay_b, arrived_b), (parts_a, pa, relay_a, arrived_a)
    ):
        ring = RingSum(copies, parts, relay, arrived, x, right, left, 256)
        parts[...] = source[...]
        ring.send_far()
        ring.send_after()
        ring.send_before()
        rings.append(ring)
    for ring in rings:
        ring.pass_on()
    give[...] = rings[0].finish(pb[x].astype(jnp.float32)).astype(jnp.bfloat16)
    swap = copies.make(give, got, mirror())
    swap.start()
    out[0] = rings[1].finish(pa[x].astype(jnp.float32)).astype(jnp.bfloat16)
    swap.wait_recv()
    out[1] = got[...]
    copies.drain_sends()


def tp_sum_kernel(terms, out, other, parts, relay, arrived, send_sems, recv_sems):
    t = lax.axis_index("tp")
    y, core = t // 2, t % 2
    right, left = y_neighbours()
    mate = sibling()
    greet((right, left, mate))
    copies = Copies(send_sems, recv_sems)
    ring = RingSum(copies, parts, relay, arrived, y, right, left, 96)
    order = (ring.far, ring.after, ring.before, y)
    given = []
    for place in order:
        copy = copies.make(terms.at[place, 1 - core], other.at[place], mate)
        copy.start()
        given.append(copy)
    for place, copy, then in zip(order, given, (ring.send_far, ring.send_after, ring.send_before)):
        copy.wait_recv()
        parts[place] = plus(terms[place, core], other[place])
        then()
    ring.pass_on()
    given[3].wait_recv()
    own = terms[y, core].astype(jnp.float32) + other[y].astype(jnp.float32)
    out[...] = ring.finish(own)
    copies.drain_sends()


def tp_gather_kernel(own, whole, send_sems, recv_sems):
    t = lax.axis_index("tp")
    y, core = t // 2, t % 2
    right, left = y_neighbours()
    mate = sibling()
    greet((right, left, mate))
    copies = Copies(send_sems, recv_sems)
    before, after, far = (y + 3) % 4, (y + 1) % 4, (y + 2) % 4
    top, low = pl.ds(0, 48), pl.ds(48, 48)
    mine = whole.at[y, core]
    sent = (
        copies.make(own.at[top], whole.at[y, core, top], right),
        copies.make(own.at[low], whole.at[y, core, low], left),
        copies.make(own.at[low], whole.at[y, core, low], right),
        copies.make(own.at[top], whole.at[y, core, top], left),
        copies.make(own, mine, mate),
    )
    for copy in sent:
        copy.start()
    whole[y, core] = own[...]
    over = [sent[4]]

    def across(block):
        copy = copies.make(block, block, mate)
        copy.start()
        over.append(copy)

    sent[0].wait_recv()
    first = whole.at[before, core, top]
    on_right = copies.make(first, first, right)
    on_right.start()
    across(first)
    sent[1].wait_recv()
    second = whole.at[after, core, low]
    on_left = copies.make(second, second, left)
    on_left.start()
    across(second)
    sent[2].wait_recv()
    across(whole.at[before, core, low])
    sent[3].wait_recv()
    across(whole.at[after, core, top])
    on_right.wait_recv()
    across(whole.at[far, core, top])
    on_left.wait_recv()
    across(whole.at[far, core, low])
    for copy in over:
        copy.wait_recv()
    copies.drain_sends()


def selector(head):
    rows = lax.broadcasted_iota(jnp.int32, (128, TILE), 0)
    pieces, rest = [], LOG2E
    for _ in range(3):
        piece = float(np.asarray(rest, dtype=jnp.bfloat16.dtype).astype(np.float64))
        pieces.append(piece)
        rest -= piece
    value = jnp.zeros((128, TILE), jnp.float32)
    for n, piece in enumerate(pieces):
        value = jnp.where(rows == 3 * head + n, piece, value)
    return value.astype(jnp.bfloat16)


HEADS = ((0, 0, 0, 64), (1, 0, 64, 64), (2, 128, 128, 128))


def attend_kernel(qa_ref, qb_ref, k_ref, ext_ref, v_ref, o_ref, tot_ref, work_ref, rhs_ref):
    z, x = sp_coords()
    kb = pl.program_id(0)

    @pl.when(kb == 0)
    def _():
        tot_ref[...] = jnp.zeros_like(tot_ref)
        for head, key_column, row, rows in HEADS:
            rhs_ref[head, 128:256, :] = selector(head)
            if rows == 64:
                rhs_ref[head, 64 - row : 128 - row, :] = jnp.zeros((64, TILE), jnp.bfloat16)

    def tile(i, q_ref, group, own_z):
        first = pl.multiple_of(i * TILE, TILE)
        columns = pl.ds(pl.multiple_of(group * 2 * BLOCK + i * TILE, TILE), TILE)

        def run(masked):
            for head, key_column, row, rows in HEADS:
                inner = row if rows == 64 else 0
                for n in range(2):
                    piece = 2 * i + n
                    rhs_ref[head, inner : inner + rows, n * 128 : (n + 1) * 128] = q_ref[
                        piece // 3, row : row + rows, pl.ds(pl.multiple_of(piece % 3 * 128, 128), 128)
                    ]
                rhs = rhs_ref[head]
                sums = jnp.zeros((8, TILE), jnp.float32)
                chunk = 128
                if masked:
                    query = lax.broadcasted_iota(jnp.int32, (1, TILE), 1) + first
                    query_pos = query + (query // HALF - x * 2 + group) * HALF
                for c in reversed(range(BLOCK // chunk)):
                    span = slice(c * chunk, (c + 1) * chunk)
                    lhs = jnp.concatenate(
                        [k_ref[0, span, key_column : key_column + 128], ext_ref[0, span, :]], axis=1
                    )
                    logit = jnp.dot(lhs, rhs, preferred_element_type=jnp.float32)
                    loss = jnp.maximum(
                        logit, jnp.log2(1.0 + jnp.exp2(jnp.minimum(logit, 100.0)))
                    )
                    if masked:
                        at = lax.broadcasted_iota(jnp.int32, (chunk, TILE), 0) + c * chunk
                        key_pos = (at % 8) * STRIPE + at // 8
                        live = key_pos < query_pos
                        loss = jnp.where(live, loss, 0.0)
                        logit = jnp.where(live, logit, -1e30)
                    for j in reversed(range(chunk // 8)):
                        eight = slice(j * 8, (j + 1) * 8)
                        sums = sums + loss[eight]
                        work_ref[c * chunk + j * 8 : c * chunk + (j + 1) * 8, :] = logit[eight] - sums
                later = [jnp.zeros((1, TILE), jnp.float32)]
                for r in range(7, 0, -1):
                    later.append(later[-1] + sums[r : r + 1])
                tot_ref[pl.ds(kb * 4 + head, 1), columns] = later[-1] + sums[0:1]
                behind = jnp.concatenate(later[::-1], axis=0)
                total = jnp.zeros((rows, TILE), jnp.float32)
                for c in range(BLOCK // 256):
                    span = slice(c * 256, (c + 1) * 256)
                    power = work_ref[span, :].reshape(32, 8, TILE) - behind[None]
                    weight = jnp.exp2(power).reshape(256, TILE).astype(jnp.bfloat16)
                    total = total + jnp.dot(
                        v_ref[0, row : row + rows, span], weight, preferred_element_type=jnp.float32
                    )
                o_ref[0, row : row + rows, columns] = total.astype(jnp.bfloat16)

        place, last = first // HALF, (first + TILE - 1) // HALF
        whole = jnp.logical_or(kb < own_z, jnp.logical_and(kb == own_z, place > x))
        none = jnp.logical_or(kb > own_z, jnp.logical_and(kb == own_z, last < x))
        partly = jnp.logical_not(jnp.logical_or(whole, none))

        @pl.when(whole)
        def _():
            run(False)

        @pl.when(partly)
        def _():
            run(True)

        @pl.when(none)
        def _():
            o_ref[0, :, columns] = jnp.zeros((256, TILE), jnp.bfloat16)

    for group, q_ref in enumerate((qa_ref, qb_ref)):

        def body(i, carry, group=group, q_ref=q_ref):
            tile(i, q_ref, group, z if group == 0 else 3 - z)
            return carry

        lax.fori_loop(0, 6, body, 0)


def attend(qa, qb, k_all, ext, v_all):
    return pl.pallas_call(
        attend_kernel,
        grid=(4,),
        in_specs=[
            pl.BlockSpec((4, 256, HALF), lambda kb: (0, 0, 0)),
            pl.BlockSpec((4, 256, HALF), lambda kb: (0, 0, 0)),
            pl.BlockSpec((1, BLOCK, 256), lambda kb: (kb, 0, 0)),
            pl.BlockSpec((1, BLOCK, 128), lambda kb: (kb, 0, 0)),
            pl.BlockSpec((1, 256, BLOCK), lambda kb: (kb, 0, 0)),
        ],
        out_specs=[
            pl.BlockSpec((1, 256, 4 * BLOCK), lambda kb: (kb, 0, 0)),
            pl.BlockSpec((16, 4 * BLOCK), lambda kb: (0, 0)),
        ],
        out_shape=[
            jax.ShapeDtypeStruct((4, 256, 4 * BLOCK), jnp.bfloat16),
            jax.ShapeDtypeStruct((16, 4 * BLOCK), jnp.float32),
        ],
        scratch_shapes=[
            pltpu.VMEM((BLOCK, TILE), jnp.float32),
            pltpu.VMEM((3, 256, TILE), jnp.bfloat16),
        ],
        compiler_params=pltpu.CompilerParams(
            dimension_semantics=("arbitrary",), vmem_limit_bytes=VMEM_LIMIT
        ),
        cost_estimate=pl.CostEstimate(
            flops=100_000_000_000, bytes_accessed=12_000_000, transcendentals=130_000_000
        ),
        name="attend",
    )(qa, qb, k_all, ext, v_all)


def combine_kernel(oa_ref, ob_ref, ta_ref, tb_ref, outa_ref, outb_ref):
    _, x = sp_coords()
    for o_ref, tot_ref, out_ref in ((oa_ref, ta_ref, outa_ref), (ob_ref, tb_ref, outb_ref)):
        nearer = jnp.zeros((4, HALF), jnp.float32)
        factors = [None] * 4
        for kb in reversed(range(4)):
            rows = slice(kb * 4, kb * 4 + 4)
            here = jnp.zeros((4, HALF), jnp.float32)
            block = jnp.zeros((4, HALF), jnp.float32)
            for other in range(4):
                term = tot_ref[other, rows, :]
                block = block + term
                here = here + jnp.where(other > x, term, 0.0)
            factors[kb] = jnp.exp2(-(nearer + here))
            nearer = nearer + block
        for head, _, row, size in HEADS:
            total = jnp.zeros((size, HALF), jnp.float32)
            for kb in range(4):
                term = o_ref[kb, row : row + size, :].astype(jnp.float32)
                total = total + term * factors[kb][head : head + 1]
            out_ref[0, row : row + size, :] = total.astype(jnp.bfloat16)


def combine(outs, totals):
    half = jax.ShapeDtypeStruct((4, 256, HALF), jnp.bfloat16)
    return pl.pallas_call(
        combine_kernel,
        grid=(4,),
        in_specs=[
            pl.BlockSpec((4, 256, HALF), lambda i: (0, 0, i)),
            pl.BlockSpec((4, 256, HALF), lambda i: (0, 0, i + 4)),
            pl.BlockSpec((4, 16, HALF), lambda i: (0, 0, i)),
            pl.BlockSpec((4, 16, HALF), lambda i: (0, 0, i + 4)),
        ],
        out_specs=[pl.BlockSpec((1, 256, HALF), lambda i: (i, 0, 0))] * 2,
        out_shape=[half, half],
        compiler_params=pltpu.CompilerParams(dimension_semantics=("arbitrary",)),
        cost_estimate=pl.CostEstimate(
            flops=4 * 256 * 3072 * 2, bytes_accessed=9_000_000, transcendentals=50_000
        ),
        name="combine",
    )(outs, outs, totals, totals)


def tp_sum(terms, collective_id, name):
    shape = (96, terms.shape[-1])
    return comm_call(
        tp_sum_kernel,
        jax.ShapeDtypeStruct(shape, jnp.float32),
        [
            pltpu.VMEM((4, *shape), jnp.bfloat16),
            pltpu.VMEM((4, *shape), jnp.bfloat16),
            pltpu.VMEM((2, 48, shape[1]), jnp.bfloat16),
            pltpu.VMEM((2, *shape), jnp.bfloat16),
        ],
        10,
        collective_id,
        name,
        (terms.reshape(4, 2, *shape),),
    )


def rounded(value):
    return lax.optimization_barrier(value.astype(jnp.bfloat16)).astype(jnp.float32)


def rms_norm(stream, gain):
    scale = lax.rsqrt(jnp.mean(stream * stream, axis=-1, keepdims=True) + 1e-06)
    return (stream * scale * gain.astype(jnp.float32)).astype(jnp.bfloat16)


def striped(value):
    return value.reshape(STRIPES, STRIPE, -1).swapaxes(0, 1).reshape(BLOCK, -1)


def on_device(
    query_small, key_small, value_small, offset_small, query_large, key_large, value_large, offset_large,
    out_small, out_large, residual, norm_gain, gate_weight, up_weight, down_weight,
):
    f32, bf16 = jnp.float32, jnp.bfloat16
    scales = np.concatenate(
        [np.full(128, LOG2E * SMALL_DIM**-0.5), np.full(128, LOG2E * LARGE_DIM**-0.5)]
    ).astype(np.float32)
    query = jnp.concatenate([query_small, query_large], axis=1).astype(f32) * scales
    query = query.astype(bf16).T
    key = striped(jnp.concatenate([key_small, key_large], axis=1))
    value = striped(jnp.concatenate([value_small, value_large], axis=1)).T
    offsets = jnp.concatenate([offset_small, offset_large], axis=0)
    offsets = offsets.reshape(3, STRIPES, STRIPE).swapaxes(1, 2).reshape(3, BLOCK)
    offsets = jnp.pad(offsets, ((0, 29), (0, 0)))
    gathered = comm_call(
        gather_kernel,
        (
            jax.ShapeDtypeStruct((4, 256, HALF), bf16),
            jax.ShapeDtypeStruct((4, 256, HALF), bf16),
            jax.ShapeDtypeStruct((4, BLOCK, 256), bf16),
            jax.ShapeDtypeStruct((4, 256, BLOCK), bf16),
            jax.ShapeDtypeStruct((4, 32, BLOCK), bf16),
        ),
        [pltpu.VMEM((256, HALF), bf16)],
        31,
        0,
        "gather_qkv",
        (query[:, :HALF], query[:, HALF:], key, value, offsets),
    )
    gate_weight, up_weight, *gathered = lax.optimization_barrier((gate_weight, up_weight, *gathered))
    qa_all, qb_all, k_all, v_all, off_all = gathered
    width = gate_weight.shape[1]
    gate_up = jnp.concatenate([gate_weight, up_weight], axis=1)
    gate_up = lax.all_gather(gate_up, "sp", axis=0, tiled=True)
    spread = np.zeros((32, 128), np.float32)
    for head in range(3):
        spread[head, 3 * head : 3 * head + 3] = 1
    ext = jnp.einsum(
        "bhs,hc->bsc", off_all, jnp.asarray(spread, bf16), preferred_element_type=f32
    ).astype(bf16)
    outs, totals = attend(qa_all, qb_all, k_all, ext, v_all)
    totals = comm_call(
        totals_kernel, jax.ShapeDtypeStruct((4, 16, 4 * BLOCK), f32), [], 6, 1, "gather_totals", (totals,)
    )
    parts_a, parts_b = combine(outs, totals)
    buffers = [pltpu.VMEM((256, HALF), bf16)] * 2
    for shape in ((4, 256, HALF), (2, 128, HALF), (2, 256, HALF)):
        buffers = [pltpu.VMEM(shape, bf16)] * 2 + buffers
    buffers = buffers[4:6] + buffers[2:4] + buffers[0:2] + buffers[6:]
    mixed = comm_call(
        x_sum_kernel,
        jax.ShapeDtypeStruct((2, 256, HALF), bf16),
        buffers,
        13,
        2,
        "sum_x",
        (parts_a, parts_b),
    )
    mixed, down_turned = lax.optimization_barrier((mixed, down_weight.T))
    down_all = lax.all_gather(down_turned, "sp", axis=0, tiled=True)
    out_weight = jnp.concatenate([out_small, out_large], axis=0)
    part = jnp.einsum("hct,cd->htd", mixed, out_weight, preferred_element_type=f32)
    attended = tp_sum(part.astype(bf16), 3, "sum_tp_mixed")
    stream = residual.astype(f32) + rounded(attended)
    normed = rms_norm(stream, norm_gain)
    rows = comm_call(
        tp_gather_kernel, jax.ShapeDtypeStruct((4, 2, 96, 2048), bf16), [], 13, 4, "gather_tp", (normed,)
    ).reshape(BLOCK, 2048)
    gate = jnp.dot(rows, gate_up[:, :width], preferred_element_type=f32)
    upper = jnp.dot(rows, gate_up[:, width:], preferred_element_type=f32)
    hidden = (jax.nn.silu(gate) * upper).astype(bf16)
    down = lax.dot_general(hidden, down_all, (((1,), (1,)), ((), ())), preferred_element_type=f32)
    summed = tp_sum(down.astype(bf16), 5, "sum_tp_down")
    return (stream + rounded(summed)).astype(bf16)


def solution(mesh):
    return jax.shard_map(
        on_device,
        mesh=mesh,
        in_specs=(
            P("sp", "tp"), P("sp", "tp"), P("sp", "tp"), P("tp", "sp"),
            P("sp", "tp"), P("sp", "tp"), P("sp", "tp"), P("tp", "sp"),
            P("tp", None), P("tp", None), P(("sp", "tp"), None), P(),
            P("sp", "tp"), P("sp", "tp"), P("tp", "sp"),
        ),
        out_specs=P(("sp", "tp"), None),
        check_vma=False,
    )
```

```python
import functools
import math

import jax
import jax.numpy as jnp
import numpy as np
from jax import lax
from jax.experimental import pallas as pl
from jax.experimental.pallas import tpu as pltpu
from jax.sharding import PartitionSpec as P

SMALL_DIM = 64
LARGE_DIM = 128
BLOCK = 768
STRIPES = 8
STRIPE = BLOCK // STRIPES
TILE = 256
HALF = BLOCK // 2
LOG2E = math.log2(math.e)
MESH = pl.DeviceIdType.MESH
VMEM_LIMIT = 60 * 1024 * 1024


def vmem():
    return pl.BlockSpec(memory_space=pltpu.VMEM)


def sp_coords():
    index = lax.axis_index("sp")
    return index // 4, index % 4


def z_neighbours():
    z, x = sp_coords()
    return {"sp": ((z + 1) % 4) * 4 + x}, {"sp": ((z + 3) % 4) * 4 + x}


def x_neighbours():
    z, x = sp_coords()
    return {"sp": z * 4 + (x + 1) % 4}, {"sp": z * 4 + (x + 3) % 4}


def mirror():
    z, x = sp_coords()
    return {"sp": (3 - z) * 4 + x}


def y_neighbours():
    t = lax.axis_index("tp")
    return {"tp": (t + 2) % 8}, {"tp": (t + 6) % 8}


def sibling():
    t = lax.axis_index("tp")
    return {"tp": t + 1 - 2 * (t % 2)}


def greet(devices):
    barrier = pltpu.get_barrier_semaphore()
    for device in devices:
        pl.semaphore_signal(barrier, inc=1, device_id=device, device_id_type=MESH)
    pl.semaphore_wait(barrier, len(devices))


class Copies:
    def __init__(self, send_sems, recv_sems):
        self.send_sems, self.recv_sems, self.used, self.all = send_sems, recv_sems, 0, []

    def make(self, src, dst, device):
        k = self.used
        self.used += 1
        copy = pltpu.make_async_remote_copy(
            src_ref=src,
            dst_ref=dst,
            send_sem=self.send_sems.at[k],
            recv_sem=self.recv_sems.at[k],
            device_id=device,
            device_id_type=MESH,
        )
        self.all.append(copy)
        return copy

    def drain_sends(self):
        for copy in self.all:
            copy.wait_send()


def hbm():
    return pl.BlockSpec(memory_space=pl.ANY)


def comm_call(kernel, outs, scratch, copies, collective_id, name, args):
    return pl.pallas_call(
        kernel,
        out_shape=[jax.ShapeDtypeStruct(shape, dtype) for shape, dtype, _ in outs],
        in_specs=[spec for _, spec in args],
        out_specs=[spec for _, _, spec in outs],
        scratch_shapes=[
            *scratch,
            pltpu.SemaphoreType.DMA((copies,)),
            pltpu.SemaphoreType.DMA((copies,)),
        ],
        compiler_params=pltpu.CompilerParams(
            collective_id=collective_id, has_side_effects=True, vmem_limit_bytes=VMEM_LIMIT
        ),
        name=name,
    )(*(array for array, _ in args))


def by_rows(ref, part):
    half = ref.shape[-2] // 2
    return ref.at[(slice(None),) * (len(ref.shape) - 2) + (pl.ds(part * half, half),)]


def by_units(ref, part):
    half = ref.shape[0] // 2
    return ref.at[pl.ds(part * half, half)]


class RingGather:
    def __init__(self, copies, own, whole, me, ring, cut=by_rows):
        self.copies, self.own, self.whole, self.me, self.ring, self.cut = copies, own, whole, me, ring, cut

    def slot(self, place, part):
        return self.cut(self.whole.at[place], part)

    def start(self):
        right, left = self.ring
        self.sent = []
        for part, device in ((0, right), (1, left), (1, right), (0, left)):
            copy = self.copies.make(self.cut(self.own, part), self.slot(self.me, part), device)
            copy.start()
            self.sent.append(copy)

    def pass_on(self):
        right, left = self.ring
        for n, (place, device) in enumerate((((self.me + 3) % 4, right), ((self.me + 1) % 4, left))):
            self.sent[n].wait_recv()
            block = self.slot(place, n)
            copy = self.copies.make(block, block, device)
            copy.start()
            self.sent.append(copy)

    def finish(self):
        for copy in self.sent[2:]:
            copy.wait_recv()


class Keep:
    def __init__(self, sems):
        self.sems, self.all = sems, []

    def start(self, src, dst):
        copy = pltpu.make_async_copy(src, dst, self.sems.at[len(self.all)])
        copy.start()
        self.all.append(copy)

    def finish(self):
        for copy in self.all:
            copy.wait()


def gather_kernel(
    q_own, q_give, k, v, off, gate, down, qa_all, qb_all, k_all, v_all, off_all, g1, d1, q_got, keep_sems,
    send_sems, recv_sems,
):
    z, x = sp_coords()
    zs, xs = z_neighbours(), x_neighbours()
    greet((*zs, *xs))
    copies, keep = Copies(send_sems, recv_sems), Keep(keep_sems)
    swap = copies.make(q_give, q_got, mirror())
    swap.start()
    first = down.at[pl.ds(0, down.shape[0] // 2)]
    jobs = [
        RingGather(copies, k, k_all, z, zs),
        RingGather(copies, v, v_all, z, zs),
        RingGather(copies, off, off_all, z, zs),
        RingGather(copies, q_own, qa_all, x, xs),
        RingGather(copies, q_got, qb_all, x, xs),
        RingGather(copies, gate, g1, x, xs),
        RingGather(copies, first, d1, x, xs),
    ]
    for n, job in enumerate(jobs):
        if n == 4:
            swap.wait_recv()
        job.start()
    keep.start(gate, g1.at[x])
    keep.start(first, d1.at[x])
    for own, whole, me in ((k, k_all, z), (v, v_all, z), (off, off_all, z), (q_own, qa_all, x), (q_got, qb_all, x)):
        whole[me] = own[...]
    for job in jobs:
        job.pass_on()
    for job in jobs:
        job.finish()
    keep.finish()
    copies.drain_sends()


def totals_kernel(tot, up, down, tot_all, u1, d2, keep_sems, send_sems, recv_sems):
    z, x = sp_coords()
    zs, xs = z_neighbours(), x_neighbours()
    greet((*zs, *xs))
    copies, keep = Copies(send_sems, recv_sems), Keep(keep_sems)
    second = down.at[pl.ds(down.shape[0] // 2, down.shape[0] // 2)]
    jobs = [
        RingGather(copies, tot, tot_all, x, xs),
        RingGather(copies, up, u1, z, zs),
        RingGather(copies, second, d2, z, zs),
    ]
    for job in jobs:
        job.start()
    keep.start(up, u1.at[z])
    keep.start(second, d2.at[z])
    tot_all[x] = tot[...]
    for job in jobs:
        job.pass_on()
    for job in jobs:
        job.finish()
    keep.finish()
    copies.drain_sends()


def plus(a, b):
    return (a.astype(jnp.float32) + b.astype(jnp.float32)).astype(jnp.bfloat16)


class RingSum:
    def __init__(self, copies, parts, relay, arrived, me, right, left, rows):
        half = rows // 2
        self.copies, self.parts, self.relay, self.arrived = copies, parts, relay, arrived
        self.me, self.right, self.left = me, right, left
        self.top, self.low = pl.ds(0, half), pl.ds(half, half)
        self.far, self.after, self.before = (me + 2) % 4, (me + 1) % 4, (me + 3) % 4
        self.waits = []

    def send(self, src, dst, device):
        copy = self.copies.make(src, dst, device)
        copy.start()
        return copy

    def send_far(self):
        self.a = self.send(self.parts.at[self.far, self.top], self.relay.at[0], self.right)
        self.b = self.send(self.parts.at[self.far, self.low], self.relay.at[1], self.left)

    def send_after(self):
        self.waits.append(
            self.send(self.parts.at[self.after, self.low], self.arrived.at[0, self.low], self.right)
        )

    def send_before(self):
        self.waits.append(
            self.send(self.parts.at[self.before, self.top], self.arrived.at[1, self.top], self.left)
        )

    def pass_on(self):
        self.a.wait_recv()
        self.parts[self.after, self.top] = plus(self.parts[self.after, self.top], self.relay[0])
        self.waits.append(
            self.send(self.parts.at[self.after, self.top], self.arrived.at[0, self.top], self.right)
        )
        self.b.wait_recv()
        self.parts[self.before, self.low] = plus(self.parts[self.before, self.low], self.relay[1])
        self.waits.append(
            self.send(self.parts.at[self.before, self.low], self.arrived.at[1, self.low], self.left)
        )

    def finish(self, own):
        for copy in self.waits:
            copy.wait_recv()
        return own + self.arrived[0].astype(jnp.float32) + self.arrived[1].astype(jnp.float32)


def x_sum_kernel(
    parts_a, parts_b, d1, out, dd1, pa, pb, relay_a, relay_b, arrived_a, arrived_b, give, got, send_sems, recv_sems
):
    z, x = sp_coords()
    right, left = x_neighbours()
    zs = z_neighbours()
    greet((right, left, *zs))
    copies = Copies(send_sems, recv_sems)
    weights = RingGather(copies, d1, dd1, z, zs, by_units)
    weights.start()
    rings = []
    for source, parts, relay, arrived in (
        (parts_b, pb, relay_b, arrived_b), (parts_a, pa, relay_a, arrived_a)
    ):
        ring = RingSum(copies, parts, relay, arrived, x, right, left, 256)
        parts[...] = source[...]
        ring.send_far()
        ring.send_after()
        ring.send_before()
        rings.append(ring)
    for ring in rings:
        ring.pass_on()
    weights.pass_on()
    give[...] = rings[0].finish(pb[x].astype(jnp.float32)).astype(jnp.bfloat16)
    swap = copies.make(give, got, mirror())
    swap.start()
    out[0] = rings[1].finish(pa[x].astype(jnp.float32)).astype(jnp.bfloat16)
    swap.wait_recv()
    out[1] = got[...]
    weights.finish()
    copies.drain_sends()


def tp_sum_kernel(with_weights, *refs):
    if with_weights:
        terms, d2, g1, u1, out, dd2, ga, ua, other, parts, relay, arrived, send_sems, recv_sems = refs
    else:
        terms, out, other, parts, relay, arrived, send_sems, recv_sems = refs
    t = lax.axis_index("tp")
    y, core = t // 2, t % 2
    right, left = y_neighbours()
    mate = sibling()
    z, x = sp_coords()
    zs, xs = z_neighbours(), x_neighbours()
    greet((right, left, mate, *zs, *xs) if with_weights else (right, left, mate))
    copies = Copies(send_sems, recv_sems)
    weights = []
    if with_weights:
        weights = [
            RingGather(copies, d2, dd2, x, xs, by_units),
            RingGather(copies, g1.at[pl.ds(0, 2)], ga, z, zs, by_units),
            RingGather(copies, u1.at[pl.ds(0, 1)], ua, x, xs),
        ]
    ring = RingSum(copies, parts, relay, arrived, y, right, left, 96)
    order = (ring.far, ring.after, ring.before, y)
    given = []
    for place in order:
        copy = copies.make(terms.at[place, 1 - core], other.at[place], mate)
        copy.start()
        given.append(copy)
    for job in weights:
        job.start()
    for place, copy, then in zip(order, given, (ring.send_far, ring.send_after, ring.send_before)):
        copy.wait_recv()
        parts[place] = plus(terms[place, core], other[place])
        then()
    ring.pass_on()
    for job in weights:
        job.pass_on()
    given[3].wait_recv()
    own = terms[y, core].astype(jnp.float32) + other[y].astype(jnp.float32)
    out[...] = ring.finish(own)
    for job in weights:
        job.finish()
    copies.drain_sends()


def tp_gather_kernel(own, g1, u1, whole, gb, ub, send_sems, recv_sems):
    t = lax.axis_index("tp")
    y, core = t // 2, t % 2
    right, left = y_neighbours()
    mate = sibling()
    z, x = sp_coords()
    zs, xs = z_neighbours(), x_neighbours()
    greet((right, left, mate, *zs, *xs))
    copies = Copies(send_sems, recv_sems)
    weights = [
        RingGather(copies, g1.at[pl.ds(2, 2)], gb, z, zs, by_units),
        RingGather(copies, u1.at[pl.ds(1, 3)], ub, x, xs),
    ]
    before, after, far = (y + 3) % 4, (y + 1) % 4, (y + 2) % 4
    top, low = pl.ds(0, 48), pl.ds(48, 48)
    mine = whole.at[y, core]
    sent = (
        copies.make(own.at[top], whole.at[y, core, top], right),
        copies.make(own.at[low], whole.at[y, core, low], left),
        copies.make(own.at[low], whole.at[y, core, low], right),
        copies.make(own.at[top], whole.at[y, core, top], left),
        copies.make(own, mine, mate),
    )
    for copy in sent:
        copy.start()
    for job in weights:
        job.start()
    whole[y, core] = own[...]
    over = [sent[4]]

    def across(block):
        copy = copies.make(block, block, mate)
        copy.start()
        over.append(copy)

    sent[0].wait_recv()
    first = whole.at[before, core, top]
    on_right = copies.make(first, first, right)
    on_right.start()
    across(first)
    sent[1].wait_recv()
    second = whole.at[after, core, low]
    on_left = copies.make(second, second, left)
    on_left.start()
    across(second)
    sent[2].wait_recv()
    across(whole.at[before, core, low])
    sent[3].wait_recv()
    across(whole.at[after, core, top])
    for job in weights:
        job.pass_on()
    on_right.wait_recv()
    across(whole.at[far, core, top])
    on_left.wait_recv()
    across(whole.at[far, core, low])
    for copy in over:
        copy.wait_recv()
    for job in weights:
        job.finish()
    copies.drain_sends()


def selector(head):
    rows = lax.broadcasted_iota(jnp.int32, (128, TILE), 0)
    pieces, rest = [], LOG2E
    for _ in range(3):
        piece = float(np.asarray(rest, dtype=jnp.bfloat16.dtype).astype(np.float64))
        pieces.append(piece)
        rest -= piece
    value = jnp.zeros((128, TILE), jnp.float32)
    for n, piece in enumerate(pieces):
        value = jnp.where(rows == 3 * head + n, piece, value)
    return value.astype(jnp.bfloat16)


HEADS = ((0, 0, 0, 64), (1, 0, 64, 64), (2, 128, 128, 128))


def attend_kernel(qa_ref, qb_ref, k_ref, ext_ref, v_ref, o_ref, tot_ref, work_ref, rhs_ref):
    z, x = sp_coords()
    kb = pl.program_id(0)

    @pl.when(kb == 0)
    def _():
        tot_ref[...] = jnp.zeros_like(tot_ref)
        for head, key_column, row, rows in HEADS:
            rhs_ref[head, 128:256, :] = selector(head)
            if rows == 64:
                rhs_ref[head, 64 - row : 128 - row, :] = jnp.zeros((64, TILE), jnp.bfloat16)

    def tile(i, q_ref, group, own_z):
        first = pl.multiple_of(i * TILE, TILE)
        columns = pl.ds(pl.multiple_of(group * 2 * BLOCK + i * TILE, TILE), TILE)

        def run(masked):
            for head, key_column, row, rows in HEADS:
                inner = row if rows == 64 else 0
                for n in range(2):
                    piece = 2 * i + n
                    rhs_ref[head, inner : inner + rows, n * 128 : (n + 1) * 128] = q_ref[
                        piece // 3, row : row + rows, pl.ds(pl.multiple_of(piece % 3 * 128, 128), 128)
                    ]
                rhs = rhs_ref[head]
                sums = jnp.zeros((8, TILE), jnp.float32)
                chunk = 128
                if masked:
                    query = lax.broadcasted_iota(jnp.int32, (1, TILE), 1) + first
                    query_pos = query + (query // HALF - x * 2 + group) * HALF
                for c in reversed(range(BLOCK // chunk)):
                    span = slice(c * chunk, (c + 1) * chunk)
                    lhs = jnp.concatenate(
                        [k_ref[0, span, key_column : key_column + 128], ext_ref[0, span, :]], axis=1
                    )
                    logit = jnp.dot(lhs, rhs, preferred_element_type=jnp.float32)
                    loss = jnp.maximum(
                        logit, jnp.log2(1.0 + jnp.exp2(jnp.minimum(logit, 100.0)))
                    )
                    if masked:
                        at = lax.broadcasted_iota(jnp.int32, (chunk, TILE), 0) + c * chunk
                        key_pos = (at % 8) * STRIPE + at // 8
                        live = key_pos < query_pos
                        loss = jnp.where(live, loss, 0.0)
                        logit = jnp.where(live, logit, -1e30)
                    for j in reversed(range(chunk // 8)):
                        eight = slice(j * 8, (j + 1) * 8)
                        sums = sums + loss[eight]
                        work_ref[c * chunk + j * 8 : c * chunk + (j + 1) * 8, :] = logit[eight] - sums
                later = [jnp.zeros((1, TILE), jnp.float32)]
                for r in range(7, 0, -1):
                    later.append(later[-1] + sums[r : r + 1])
                tot_ref[pl.ds(kb * 4 + head, 1), columns] = later[-1] + sums[0:1]
                behind = jnp.concatenate(later[::-1], axis=0)
                total = jnp.zeros((rows, TILE), jnp.float32)
                for c in range(BLOCK // 256):
                    span = slice(c * 256, (c + 1) * 256)
                    power = work_ref[span, :].reshape(32, 8, TILE) - behind[None]
                    weight = jnp.exp2(power).reshape(256, TILE).astype(jnp.bfloat16)
                    total = total + jnp.dot(
                        v_ref[0, row : row + rows, span], weight, preferred_element_type=jnp.float32
                    )
                o_ref[0, row : row + rows, columns] = total.astype(jnp.bfloat16)

        place, last = first // HALF, (first + TILE - 1) // HALF
        whole = jnp.logical_or(kb < own_z, jnp.logical_and(kb == own_z, place > x))
        none = jnp.logical_or(kb > own_z, jnp.logical_and(kb == own_z, last < x))
        partly = jnp.logical_not(jnp.logical_or(whole, none))

        @pl.when(whole)
        def _():
            run(False)

        @pl.when(partly)
        def _():
            run(True)

        @pl.when(none)
        def _():
            o_ref[0, :, columns] = jnp.zeros((256, TILE), jnp.bfloat16)

    for group, q_ref in enumerate((qa_ref, qb_ref)):

        def body(i, carry, group=group, q_ref=q_ref):
            tile(i, q_ref, group, z if group == 0 else 3 - z)
            return carry

        lax.fori_loop(0, 6, body, 0)


def attend(qa, qb, k_all, ext, v_all):
    return pl.pallas_call(
        attend_kernel,
        grid=(4,),
        in_specs=[
            pl.BlockSpec((4, 256, HALF), lambda kb: (0, 0, 0)),
            pl.BlockSpec((4, 256, HALF), lambda kb: (0, 0, 0)),
            pl.BlockSpec((1, BLOCK, 256), lambda kb: (kb, 0, 0)),
            pl.BlockSpec((1, BLOCK, 128), lambda kb: (kb, 0, 0)),
            pl.BlockSpec((1, 256, BLOCK), lambda kb: (kb, 0, 0)),
        ],
        out_specs=[
            pl.BlockSpec((1, 256, 4 * BLOCK), lambda kb: (kb, 0, 0)),
            pl.BlockSpec((16, 4 * BLOCK), lambda kb: (0, 0)),
        ],
        out_shape=[
            jax.ShapeDtypeStruct((4, 256, 4 * BLOCK), jnp.bfloat16),
            jax.ShapeDtypeStruct((16, 4 * BLOCK), jnp.float32),
        ],
        scratch_shapes=[
            pltpu.VMEM((BLOCK, TILE), jnp.float32),
            pltpu.VMEM((3, 256, TILE), jnp.bfloat16),
        ],
        compiler_params=pltpu.CompilerParams(
            dimension_semantics=("arbitrary",), vmem_limit_bytes=VMEM_LIMIT
        ),
        cost_estimate=pl.CostEstimate(
            flops=100_000_000_000, bytes_accessed=12_000_000, transcendentals=130_000_000
        ),
        name="attend",
    )(qa, qb, k_all, ext, v_all)


def combine_kernel(oa_ref, ob_ref, ta_ref, tb_ref, outa_ref, outb_ref):
    _, x = sp_coords()
    for o_ref, tot_ref, out_ref in ((oa_ref, ta_ref, outa_ref), (ob_ref, tb_ref, outb_ref)):
        nearer = jnp.zeros((4, HALF), jnp.float32)
        factors = [None] * 4
        for kb in reversed(range(4)):
            rows = slice(kb * 4, kb * 4 + 4)
            here = jnp.zeros((4, HALF), jnp.float32)
            block = jnp.zeros((4, HALF), jnp.float32)
            for other in range(4):
                term = tot_ref[other, rows, :]
                block = block + term
                here = here + jnp.where(other > x, term, 0.0)
            factors[kb] = jnp.exp2(-(nearer + here))
            nearer = nearer + block
        for head, _, row, size in HEADS:
            total = jnp.zeros((size, HALF), jnp.float32)
            for kb in range(4):
                term = o_ref[kb, row : row + size, :].astype(jnp.float32)
                total = total + term * factors[kb][head : head + 1]
            out_ref[0, row : row + size, :] = total.astype(jnp.bfloat16)


def combine(outs, totals):
    half = jax.ShapeDtypeStruct((4, 256, HALF), jnp.bfloat16)
    return pl.pallas_call(
        combine_kernel,
        grid=(4,),
        in_specs=[
            pl.BlockSpec((4, 256, HALF), lambda i: (0, 0, i)),
            pl.BlockSpec((4, 256, HALF), lambda i: (0, 0, i + 4)),
            pl.BlockSpec((4, 16, HALF), lambda i: (0, 0, i)),
            pl.BlockSpec((4, 16, HALF), lambda i: (0, 0, i + 4)),
        ],
        out_specs=[pl.BlockSpec((1, 256, HALF), lambda i: (i, 0, 0))] * 2,
        out_shape=[half, half],
        compiler_params=pltpu.CompilerParams(dimension_semantics=("arbitrary",)),
        cost_estimate=pl.CostEstimate(
            flops=4 * 256 * 3072 * 2, bytes_accessed=9_000_000, transcendentals=50_000
        ),
        name="combine",
    )(outs, outs, totals, totals)


def tp_sum(terms, collective_id, name, weights=()):
    shape = (96, terms.shape[-1])
    bf16 = jnp.bfloat16
    outs, args = [(shape, jnp.float32, vmem())], [(terms.reshape(4, 2, *shape), vmem())]
    if weights:
        d2, g1, u1 = weights
        args += [(array, hbm()) for array in weights]
        outs += [
            ((4, *d2.shape), bf16, hbm()),
            ((4, 2, *g1.shape[1:]), bf16, hbm()),
            ((4, 1, *u1.shape[1:]), bf16, hbm()),
        ]
    out = comm_call(
        functools.partial(tp_sum_kernel, bool(weights)),
        outs,
        [
            pltpu.VMEM((4, *shape), bf16),
            pltpu.VMEM((4, *shape), bf16),
            pltpu.VMEM((2, 48, shape[1]), bf16),
            pltpu.VMEM((2, *shape), bf16),
        ],
        28 if weights else 10,
        collective_id,
        name,
        args,
    )
    return out if weights else out[0]


def feed_kernel(
    rows, g1, ga, gb, u1, ua, ub, d1, dd1, d2, dd2, out, r_vmem, gate_w, up_w, down_w, gate, hidden, sems
):
    z, x = sp_coords()
    half = d1.shape[1]
    row_copy = pltpu.make_async_copy(rows, r_vmem, sems.at[64])
    row_copy.start()
    waits = [[], [], []]

    def fetch(stage, mine, own, other, dst, n):
        kept = pltpu.make_async_copy(own, dst, sems.at[n])
        came = pltpu.make_async_copy(other, dst, sems.at[n])
        pl.when(mine)(kept.start)
        pl.when(jnp.logical_not(mine))(came.start)
        waits[stage].append(came)

    spots = [(zp, xp, pl.ds((zp * 4 + xp) * 128, 128)) for zp in range(4) for xp in range(4)]
    for n, (zp, xp, lanes) in enumerate(spots):
        fetch(0, z == zp, g1.at[xp], (ga, gb)[xp // 2].at[zp, xp % 2], gate_w.at[:, lanes], n)
    for n, (zp, xp, lanes) in enumerate(spots):
        other = ua.at[xp, 0] if zp == 0 else ub.at[xp, zp - 1]
        fetch(1, x == xp, u1.at[zp], other, up_w.at[:, lanes], 16 + n)
    for n, (zp, xp, lanes) in enumerate(spots):
        fetch(2, z == zp, d1.at[xp], dd1.at[zp, xp], down_w.at[pl.ds(0, half), lanes], 32 + n)
        fetch(2, x == xp, d2.at[zp], dd2.at[xp, zp], down_w.at[pl.ds(half, half), lanes], 48 + n)
    turned = (((1,), (1,)), ((), ()))

    def over_rows(step):
        lax.fori_loop(0, 3, lambda i, c: (step(pl.ds(pl.multiple_of(i * 256, 256), 256)), c)[1], 0)

    row_copy.wait()
    for copy in waits[0]:
        copy.wait()

    def gates(span):
        gate[span, :] = lax.dot_general(
            r_vmem[span, :], gate_w[...], turned, preferred_element_type=jnp.float32
        )

    over_rows(gates)
    for copy in waits[1]:
        copy.wait()

    def hide(span):
        upper = lax.dot_general(
            r_vmem[span, :], up_w[...], turned, preferred_element_type=jnp.float32
        )
        value = gate[span, :]
        hidden[span, :] = (value / (1.0 + jnp.exp(-value)) * upper).astype(jnp.bfloat16)

    over_rows(hide)
    for copy in waits[2]:
        copy.wait()

    def lower(span):
        out[span, :] = jnp.dot(
            hidden[span, :], down_w[...], preferred_element_type=jnp.float32
        ).astype(jnp.bfloat16)

    over_rows(lower)


def feed(rows, *weights):
    units = weights[0].shape[1]
    bf16 = jnp.bfloat16
    return pl.pallas_call(
        feed_kernel,
        out_shape=jax.ShapeDtypeStruct((BLOCK, 2048), bf16),
        in_specs=[hbm()] * (1 + len(weights)),
        out_specs=vmem(),
        scratch_shapes=[
            pltpu.VMEM((BLOCK, 2048), bf16),
            pltpu.VMEM((units, 2048), bf16),
            pltpu.VMEM((units, 2048), bf16),
            pltpu.VMEM((units, 2048), bf16),
            pltpu.VMEM((BLOCK, units), jnp.float32),
            pltpu.VMEM((BLOCK, units), bf16),
            pltpu.SemaphoreType.DMA((65,)),
        ],
        compiler_params=pltpu.CompilerParams(vmem_limit_bytes=VMEM_LIMIT),
        cost_estimate=pl.CostEstimate(
            flops=6 * BLOCK * 2048 * units, bytes_accessed=15_000_000, transcendentals=BLOCK * units
        ),
        name="feed",
    )(rows, *weights)


def rounded(value):
    return lax.optimization_barrier(value.astype(jnp.bfloat16)).astype(jnp.float32)


def rms_norm(stream, gain):
    scale = lax.rsqrt(jnp.mean(stream * stream, axis=-1, keepdims=True) + 1e-06)
    return (stream * scale * gain.astype(jnp.float32)).astype(jnp.bfloat16)


def striped(value):
    return value.reshape(STRIPES, STRIPE, -1).swapaxes(0, 1).reshape(BLOCK, -1)


def on_device(
    query_small, key_small, value_small, offset_small, query_large, key_large, value_large, offset_large,
    out_small, out_large, residual, norm_gain, gate_weight, up_weight, down_weight,
):
    f32, bf16 = jnp.float32, jnp.bfloat16
    scales = np.concatenate(
        [np.full(128, LOG2E * SMALL_DIM**-0.5), np.full(128, LOG2E * LARGE_DIM**-0.5)]
    ).astype(np.float32)
    query = jnp.concatenate([query_small, query_large], axis=1).astype(f32) * scales
    query = query.astype(bf16).T
    key = striped(jnp.concatenate([key_small, key_large], axis=1))
    value = striped(jnp.concatenate([value_small, value_large], axis=1)).T
    offsets = jnp.concatenate([offset_small, offset_large], axis=0)
    offsets = offsets.reshape(3, STRIPES, STRIPE).swapaxes(1, 2).reshape(3, BLOCK)
    offsets = jnp.pad(offsets, ((0, 29), (0, 0)))
    gate, up, down = gate_weight.T, up_weight.T, down_weight
    units = down.shape[0]
    qa_all, qb_all, k_all, v_all, off_all, g1, d1 = comm_call(
        gather_kernel,
        [
            ((4, 256, HALF), bf16, vmem()),
            ((4, 256, HALF), bf16, vmem()),
            ((4, BLOCK, 256), bf16, vmem()),
            ((4, 256, BLOCK), bf16, vmem()),
            ((4, 32, BLOCK), bf16, vmem()),
            ((4, units, 128), bf16, hbm()),
            ((4, units // 2, 128), bf16, hbm()),
        ],
        [pltpu.VMEM((256, HALF), bf16), pltpu.SemaphoreType.DMA((2,))],
        43,
        0,
        "gather_qkv",
        [(array, vmem()) for array in (query[:, :HALF], query[:, HALF:], key, value, offsets, gate, down)],
    )
    spread = np.zeros((32, 128), np.float32)
    for head in range(3):
        spread[head, 3 * head : 3 * head + 3] = 1
    ext = jnp.einsum(
        "bhs,hc->bsc", off_all, jnp.asarray(spread, bf16), preferred_element_type=f32
    ).astype(bf16)
    outs, totals = attend(qa_all, qb_all, k_all, ext, v_all)
    totals, u1, d2 = comm_call(
        totals_kernel,
        [
            ((4, 16, 4 * BLOCK), f32, vmem()),
            ((4, units, 128), bf16, hbm()),
            ((4, units // 2, 128), bf16, hbm()),
        ],
        [pltpu.SemaphoreType.DMA((2,))],
        18,
        1,
        "gather_totals",
        [(array, vmem()) for array in (totals, up, down)],
    )
    parts_a, parts_b = combine(outs, totals)
    buffers = [pltpu.VMEM((256, HALF), bf16)] * 2
    for shape in ((4, 256, HALF), (2, 128, HALF), (2, 256, HALF)):
        buffers = [pltpu.VMEM(shape, bf16)] * 2 + buffers
    buffers = buffers[4:6] + buffers[2:4] + buffers[0:2] + buffers[6:]
    mixed, dd1 = comm_call(
        x_sum_kernel,
        [((2, 256, HALF), bf16, vmem()), ((4, *d1.shape), bf16, hbm())],
        buffers,
        19,
        2,
        "sum_x",
        [(parts_a, vmem()), (parts_b, vmem()), (d1, hbm())],
    )
    out_weight = jnp.concatenate([out_small, out_large], axis=0)
    part = jnp.einsum("hct,cd->htd", mixed, out_weight, preferred_element_type=f32)
    attended, dd2, ga, ua = tp_sum(part.astype(bf16), 3, "sum_tp_mixed", (d2, g1, u1))
    stream = residual.astype(f32) + rounded(attended)
    normed = rms_norm(stream, norm_gain)
    rows, gb, ub = comm_call(
        tp_gather_kernel,
        [
            ((4, 2, 96, 2048), bf16, vmem()),
            ((4, 2, *g1.shape[1:]), bf16, hbm()),
            ((4, 3, *u1.shape[1:]), bf16, hbm()),
        ],
        [],
        25,
        4,
        "gather_tp",
        [(normed, vmem()), (g1, hbm()), (u1, hbm())],
    )
    down = feed(rows.reshape(BLOCK, 2048), g1, ga, gb, u1, ua, ub, d1, dd1, d2, dd2)
    summed = tp_sum(down, 5, "sum_tp_down")
    return (stream + rounded(summed)).astype(bf16)


def solution(mesh):
    return jax.shard_map(
        on_device,
        mesh=mesh,
        in_specs=(
            P("sp", "tp"), P("sp", "tp"), P("sp", "tp"), P("tp", "sp"),
            P("sp", "tp"), P("sp", "tp"), P("sp", "tp"), P("tp", "sp"),
            P("tp", None), P("tp", None), P(("sp", "tp"), None), P(),
            P("sp", "tp"), P("sp", "tp"), P("tp", "sp"),
        ),
        out_specs=P(("sp", "tp"), None),
        check_vma=False,
    )
```

```python
import functools
import math

import jax
import jax.numpy as jnp
import numpy as np
from jax import lax
from jax.experimental import pallas as pl
from jax.experimental.pallas import tpu as pltpu
from jax.sharding import PartitionSpec as P

SMALL_DIM = 64
LARGE_DIM = 128
BLOCK = 768
STRIPES = 8
STRIPE = BLOCK // STRIPES
TILE = 256
HALF = BLOCK // 2
LOG2E = math.log2(math.e)
MESH = pl.DeviceIdType.MESH
VMEM_LIMIT = 60 * 1024 * 1024


def vmem():
    return pl.BlockSpec(memory_space=pltpu.VMEM)


def sp_coords():
    index = lax.axis_index("sp")
    return index // 4, index % 4


def z_neighbours():
    z, x = sp_coords()
    return {"sp": ((z + 1) % 4) * 4 + x}, {"sp": ((z + 3) % 4) * 4 + x}


def x_neighbours():
    z, x = sp_coords()
    return {"sp": z * 4 + (x + 1) % 4}, {"sp": z * 4 + (x + 3) % 4}


def mirror():
    z, x = sp_coords()
    return {"sp": (3 - z) * 4 + x}


def y_neighbours():
    t = lax.axis_index("tp")
    return {"tp": (t + 2) % 8}, {"tp": (t + 6) % 8}


def sibling():
    t = lax.axis_index("tp")
    return {"tp": t + 1 - 2 * (t % 2)}


def greet(devices):
    barrier = pltpu.get_barrier_semaphore()
    for device in devices:
        pl.semaphore_signal(barrier, inc=1, device_id=device, device_id_type=MESH)
    pl.semaphore_wait(barrier, len(devices))


class Copies:
    def __init__(self, send_sems, recv_sems):
        self.send_sems, self.recv_sems, self.used, self.all = send_sems, recv_sems, 0, []

    def make(self, src, dst, device):
        k = self.used
        self.used += 1
        copy = pltpu.make_async_remote_copy(
            src_ref=src,
            dst_ref=dst,
            send_sem=self.send_sems.at[k],
            recv_sem=self.recv_sems.at[k],
            device_id=device,
            device_id_type=MESH,
        )
        self.all.append(copy)
        return copy

    def drain_sends(self):
        for copy in self.all:
            copy.wait_send()


def hbm():
    return pl.BlockSpec(memory_space=pl.ANY)


def comm_call(kernel, outs, scratch, copies, collective_id, name, args):
    return pl.pallas_call(
        kernel,
        out_shape=[jax.ShapeDtypeStruct(shape, dtype) for shape, dtype, _ in outs],
        in_specs=[spec for _, spec in args],
        out_specs=[spec for _, _, spec in outs],
        scratch_shapes=[
            *scratch,
            pltpu.SemaphoreType.DMA((copies,)),
            pltpu.SemaphoreType.DMA((copies,)),
        ],
        compiler_params=pltpu.CompilerParams(
            collective_id=collective_id, has_side_effects=True, vmem_limit_bytes=VMEM_LIMIT
        ),
        name=name,
    )(*(array for array, _ in args))


def by_rows(ref, part):
    half = ref.shape[-2] // 2
    return ref.at[(slice(None),) * (len(ref.shape) - 2) + (pl.ds(part * half, half),)]


def by_units(ref, part):
    half = ref.shape[0] // 2
    return ref.at[pl.ds(part * half, half)]


class RingGather:
    def __init__(self, copies, own, whole, me, ring, cut=by_rows):
        self.copies, self.own, self.whole, self.me, self.ring, self.cut = copies, own, whole, me, ring, cut

    def slot(self, place, part):
        return self.cut(self.whole.at[place], part)

    def start(self):
        right, left = self.ring
        self.sent = []
        for part, device in ((0, right), (1, left), (1, right), (0, left)):
            copy = self.copies.make(self.cut(self.own, part), self.slot(self.me, part), device)
            copy.start()
            self.sent.append(copy)

    def pass_on(self):
        right, left = self.ring
        for n, (place, device) in enumerate((((self.me + 3) % 4, right), ((self.me + 1) % 4, left))):
            self.sent[n].wait_recv()
            block = self.slot(place, n)
            copy = self.copies.make(block, block, device)
            copy.start()
            self.sent.append(copy)

    def finish(self):
        for copy in self.sent[2:]:
            copy.wait_recv()


class Keep:
    def __init__(self, sems):
        self.sems, self.all = sems, []

    def start(self, src, dst):
        copy = pltpu.make_async_copy(src, dst, self.sems.at[len(self.all)])
        copy.start()
        self.all.append(copy)

    def finish(self):
        for copy in self.all:
            copy.wait()


def gather_kernel(
    q_own, q_give, k, v, off, gate, down, qa_all, qb_all, k_all, v_all, off_all, g1, d1, q_got, keep_sems,
    send_sems, recv_sems,
):
    z, x = sp_coords()
    zs, xs = z_neighbours(), x_neighbours()
    greet((*zs, *xs))
    copies, keep = Copies(send_sems, recv_sems), Keep(keep_sems)
    swap = copies.make(q_give, q_got, mirror())
    swap.start()
    first = down.at[pl.ds(0, down.shape[0] // 2)]
    jobs = [
        RingGather(copies, k, k_all, z, zs),
        RingGather(copies, v, v_all, z, zs),
        RingGather(copies, off, off_all, z, zs),
        RingGather(copies, q_own, qa_all, x, xs),
        RingGather(copies, q_got, qb_all, x, xs),
        RingGather(copies, gate, g1, x, xs),
        RingGather(copies, first, d1, x, xs),
    ]
    for n, job in enumerate(jobs):
        if n == 4:
            swap.wait_recv()
        job.start()
    keep.start(gate, g1.at[x])
    keep.start(first, d1.at[x])
    for own, whole, me in ((k, k_all, z), (v, v_all, z), (off, off_all, z), (q_own, qa_all, x), (q_got, qb_all, x)):
        whole[me] = own[...]
    for job in jobs:
        job.pass_on()
    for job in jobs:
        job.finish()
    keep.finish()
    copies.drain_sends()


def plus(a, b):
    return (a.astype(jnp.float32) + b.astype(jnp.float32)).astype(jnp.bfloat16)


class RingSum:
    def __init__(self, copies, parts, relay, arrived, me, right, left, rows):
        half = rows // 2
        self.copies, self.parts, self.relay, self.arrived = copies, parts, relay, arrived
        self.me, self.right, self.left = me, right, left
        self.top, self.low = pl.ds(0, half), pl.ds(half, half)
        self.far, self.after, self.before = (me + 2) % 4, (me + 1) % 4, (me + 3) % 4
        self.waits = []

    def send(self, src, dst, device):
        copy = self.copies.make(src, dst, device)
        copy.start()
        return copy

    def send_far(self):
        self.a = self.send(self.parts.at[self.far, self.top], self.relay.at[0], self.right)
        self.b = self.send(self.parts.at[self.far, self.low], self.relay.at[1], self.left)

    def send_after(self):
        self.waits.append(
            self.send(self.parts.at[self.after, self.low], self.arrived.at[0, self.low], self.right)
        )

    def send_before(self):
        self.waits.append(
            self.send(self.parts.at[self.before, self.top], self.arrived.at[1, self.top], self.left)
        )

    def pass_on(self):
        self.a.wait_recv()
        self.parts[self.after, self.top] = plus(self.parts[self.after, self.top], self.relay[0])
        self.waits.append(
            self.send(self.parts.at[self.after, self.top], self.arrived.at[0, self.top], self.right)
        )
        self.b.wait_recv()
        self.parts[self.before, self.low] = plus(self.parts[self.before, self.low], self.relay[1])
        self.waits.append(
            self.send(self.parts.at[self.before, self.low], self.arrived.at[1, self.low], self.left)
        )

    def finish(self, own):
        for copy in self.waits:
            copy.wait_recv()
        return own + self.arrived[0].astype(jnp.float32) + self.arrived[1].astype(jnp.float32)


def scaled(o_ref, tot_ref, x, columns):
    nearer = jnp.zeros((4, HALF), jnp.float32)
    factors = [None] * 4
    for kb in reversed(range(4)):
        here = jnp.zeros((4, HALF), jnp.float32)
        block = jnp.zeros((4, HALF), jnp.float32)
        for other in range(4):
            term = tot_ref[other, kb * 4 : kb * 4 + 4, columns]
            block = block + term
            here = here + jnp.where(other > x, term, 0.0)
        factors[kb] = jnp.exp2(-(nearer + here))
        nearer = nearer + block
    pieces = []
    for head, _, row, size in HEADS:
        total = jnp.zeros((size, HALF), jnp.float32)
        for kb in range(4):
            term = o_ref[kb, row : row + size, columns].astype(jnp.float32)
            total = total + term * factors[kb][head : head + 1]
        pieces.append(total)
    return jnp.concatenate(pieces, axis=0)


def mix_kernel(
    tot, up, down, o_hbm, out, u1, d2, tot_all, o_ref, pa, pb, relay_a, relay_b, arrived_a, arrived_b, give, got,
    keep_sems, load_sems, send_sems, recv_sems,
):
    z, x = sp_coords()
    zs, xs = z_neighbours(), x_neighbours()
    greet((*zs, *xs))
    copies, keep = Copies(send_sems, recv_sems), Keep(keep_sems)
    second = down.at[pl.ds(down.shape[0] // 2, down.shape[0] // 2)]
    totals = RingGather(copies, tot, tot_all, x, xs)
    weights = [RingGather(copies, up, u1, z, zs), RingGather(copies, second, d2, z, zs)]
    totals.start()
    for job in weights:
        job.start()
    keep.start(up, u1.at[z])
    keep.start(second, d2.at[z])
    rings = [
        RingSum(copies, parts, relay, arrived, x, *xs, 256)
        for parts, relay, arrived in ((pb, relay_b, arrived_b), (pa, relay_a, arrived_a))
    ]

    def columns(group, place):
        return pl.ds(pl.multiple_of((group * 4 + place) * HALF, 128), HALF)

    loads = {}
    for n, (ring, group) in enumerate(zip(rings, (1, 0))):
        for m, place in enumerate((ring.far, ring.after, ring.before, x)):
            span = columns(group, place)
            loads[n, m] = pltpu.make_async_copy(
                o_hbm.at[:, :, span], o_ref.at[:, :, span], load_sems.at[n * 4 + m]
            )
            loads[n, m].start()
    tot_all[x] = tot[...]
    totals.pass_on()
    totals.finish()
    for n, (ring, group) in enumerate(zip(rings, (1, 0))):
        sends = (ring.send_far, ring.send_after, ring.send_before)
        for m, (place, send) in enumerate(zip((ring.far, ring.after, ring.before), sends)):
            loads[n, m].wait()
            ring.parts[place] = scaled(o_ref, tot_all, x, columns(group, place)).astype(jnp.bfloat16)
            send()
    for job in weights:
        job.pass_on()
    for ring in rings:
        ring.pass_on()
    loads[0, 3].wait()
    give[...] = rings[0].finish(scaled(o_ref, tot_all, x, columns(1, x))).astype(jnp.bfloat16)
    swap = copies.make(give, got, mirror())
    swap.start()
    loads[1, 3].wait()
    out[0] = rings[1].finish(scaled(o_ref, tot_all, x, columns(0, x))).astype(jnp.bfloat16)
    for job in weights:
        job.finish()
    keep.finish()
    swap.wait_recv()
    out[1] = got[...]
    copies.drain_sends()


def pair_sum(copies, terms, other, ring, y, core, mate):
    order = (ring.far, ring.after, ring.before, y)
    given = []
    for place in order:
        copy = copies.make(terms.at[place, 1 - core], other.at[place], mate)
        copy.start()
        given.append(copy)
    for place, copy, then in zip(order, given, (ring.send_far, ring.send_after, ring.send_before)):
        copy.wait_recv()
        ring.parts[place] = plus(terms[place, core], other[place])
        then()
    ring.pass_on()
    given[3].wait_recv()
    return terms[y, core].astype(jnp.float32) + other[y].astype(jnp.float32)


def tp_place():
    t = lax.axis_index("tp")
    return t // 2, t % 2


def tp_sum_kernel(terms, out, other, parts, relay, arrived, send_sems, recv_sems):
    y, core = tp_place()
    ys, mate = y_neighbours(), sibling()
    greet((*ys, mate))
    copies = Copies(send_sems, recv_sems)
    ring = RingSum(copies, parts, relay, arrived, y, *ys, 96)
    own = pair_sum(copies, terms, other, ring, y, core, mate)
    out[...] = ring.finish(own)
    copies.drain_sends()


def middle_kernel(
    terms, residual, gain, d1, d2, g1, u1, stream, whole, dd1, dd2, gg, uu, other, parts, relay, arrived, own,
    send_sems, recv_sems,
):
    z, x = sp_coords()
    y, core = tp_place()
    zs, xs, ys, mate = z_neighbours(), x_neighbours(), y_neighbours(), sibling()
    greet((*ys, mate, *zs, *xs))
    copies = Copies(send_sems, recv_sems)
    early = [
        RingGather(copies, d2, dd2, x, xs, by_units),
        RingGather(copies, d1, dd1, z, zs, by_units),
    ]
    late = [
        RingGather(copies, u1, uu, x, xs, by_units),
        RingGather(copies, g1, gg, z, zs, by_units),
    ]
    ring = RingSum(copies, parts, relay, arrived, y, *ys, 96)
    for job in early + late:
        job.start()
    total = pair_sum(copies, terms, other, ring, y, core, mate)
    for job in early:
        job.pass_on()
    attended = ring.finish(total).astype(jnp.bfloat16).astype(jnp.float32)
    value = residual[...].astype(jnp.float32) + attended
    stream[...] = value
    scale = lax.rsqrt(jnp.mean(value * value, axis=-1, keepdims=True) + 1e-06)
    own[...] = (value * scale * gain[...].astype(jnp.float32)).astype(jnp.bfloat16)

    right, left = ys
    before, after, far = (y + 3) % 4, (y + 1) % 4, (y + 2) % 4
    top, low = pl.ds(0, 48), pl.ds(48, 48)
    sent = (
        copies.make(own.at[top], whole.at[y, core, top], right),
        copies.make(own.at[low], whole.at[y, core, low], left),
        copies.make(own.at[low], whole.at[y, core, low], right),
        copies.make(own.at[top], whole.at[y, core, top], left),
        copies.make(own, whole.at[y, core], mate),
    )
    for copy in sent:
        copy.start()
    whole[y, core] = own[...]
    over = [sent[4]]

    def send(block, device):
        copy = copies.make(block, block, device)
        copy.start()
        return copy

    sent[0].wait_recv()
    on_right = send(whole.at[before, core, top], right)
    over.append(send(whole.at[before, core, top], mate))
    sent[1].wait_recv()
    on_left = send(whole.at[after, core, low], left)
    over.append(send(whole.at[after, core, low], mate))
    for job in late:
        job.pass_on()
    sent[2].wait_recv()
    over.append(send(whole.at[before, core, low], mate))
    sent[3].wait_recv()
    over.append(send(whole.at[after, core, top], mate))
    on_right.wait_recv()
    over.append(send(whole.at[far, core, top], mate))
    on_left.wait_recv()
    over.append(send(whole.at[far, core, low], mate))
    for copy in over:
        copy.wait_recv()
    for job in early + late:
        job.finish()
    copies.drain_sends()


HEADS = ((0, 0, 0, 64), (1, 0, 64, 64), (2, 128, 128, 128))


def selector(head):
    rows = lax.broadcasted_iota(jnp.int32, (128, TILE), 0)
    pieces, rest = [], LOG2E
    for _ in range(3):
        piece = float(np.asarray(rest, dtype=jnp.bfloat16.dtype).astype(np.float64))
        pieces.append(piece)
        rest -= piece
    value = jnp.zeros((128, TILE), jnp.float32)
    for n, piece in enumerate(pieces):
        value = jnp.where(rows == 3 * head + n, piece, value)
    return value.astype(jnp.bfloat16)


def attend_kernel(qa_ref, qb_ref, k_ref, ext_ref, v_ref, o_ref, tot_ref, work_ref, rhs_ref):
    z, x = sp_coords()
    kb = pl.program_id(0)

    @pl.when(kb == 0)
    def _():
        tot_ref[...] = jnp.zeros_like(tot_ref)
        for head, key_column, row, rows in HEADS:
            rhs_ref[head, 128:256, :] = selector(head)
            if rows == 64:
                rhs_ref[head, 64 - row : 128 - row, :] = jnp.zeros((64, TILE), jnp.bfloat16)

    def tile(i, q_ref, group, own_z):
        first = pl.multiple_of(i * TILE, TILE)
        columns = pl.ds(pl.multiple_of(group * 2 * BLOCK + i * TILE, TILE), TILE)

        def run(masked):
            for head, key_column, row, rows in HEADS:
                inner = row if rows == 64 else 0
                for n in range(2):
                    piece = 2 * i + n
                    rhs_ref[head, inner : inner + rows, n * 128 : (n + 1) * 128] = q_ref[
                        piece // 3, row : row + rows, pl.ds(pl.multiple_of(piece % 3 * 128, 128), 128)
                    ]
                rhs = rhs_ref[head]
                sums = jnp.zeros((8, TILE), jnp.float32)
                chunk = 128
                if masked:
                    query = lax.broadcasted_iota(jnp.int32, (1, TILE), 1) + first
                    query_pos = query + (query // HALF - x * 2 + group) * HALF
                for c in reversed(range(BLOCK // chunk)):
                    span = slice(c * chunk, (c + 1) * chunk)
                    lhs = jnp.concatenate(
                        [k_ref[0, span, key_column : key_column + 128], ext_ref[0, span, :]], axis=1
                    )
                    logit = jnp.dot(lhs, rhs, preferred_element_type=jnp.float32)
                    loss = jnp.maximum(
                        logit, jnp.log2(1.0 + jnp.exp2(jnp.minimum(logit, 100.0)))
                    )
                    if masked:
                        at = lax.broadcasted_iota(jnp.int32, (chunk, TILE), 0) + c * chunk
                        key_pos = (at % 8) * STRIPE + at // 8
                        live = key_pos < query_pos
                        loss = jnp.where(live, loss, 0.0)
                        logit = jnp.where(live, logit, -1e30)
                    for j in reversed(range(chunk // 8)):
                        eight = slice(j * 8, (j + 1) * 8)
                        sums = sums + loss[eight]
                        work_ref[c * chunk + j * 8 : c * chunk + (j + 1) * 8, :] = logit[eight] - sums
                later = [jnp.zeros((1, TILE), jnp.float32)]
                for r in range(7, 0, -1):
                    later.append(later[-1] + sums[r : r + 1])
                tot_ref[pl.ds(kb * 4 + head, 1), columns] = later[-1] + sums[0:1]
                behind = jnp.concatenate(later[::-1], axis=0)
                total = jnp.zeros((rows, TILE), jnp.float32)
                for c in range(BLOCK // 256):
                    span = slice(c * 256, (c + 1) * 256)
                    power = work_ref[span, :].reshape(32, 8, TILE) - behind[None]
                    weight = jnp.exp2(power).reshape(256, TILE).astype(jnp.bfloat16)
                    total = total + jnp.dot(
                        v_ref[0, row : row + rows, span], weight, preferred_element_type=jnp.float32
                    )
                o_ref[0, row : row + rows, columns] = total.astype(jnp.bfloat16)

        place, last = first // HALF, (first + TILE - 1) // HALF
        whole = jnp.logical_or(kb < own_z, jnp.logical_and(kb == own_z, place > x))
        none = jnp.logical_or(kb > own_z, jnp.logical_and(kb == own_z, last < x))
        partly = jnp.logical_not(jnp.logical_or(whole, none))

        @pl.when(whole)
        def _():
            run(False)

        @pl.when(partly)
        def _():
            run(True)

        @pl.when(none)
        def _():
            o_ref[0, :, columns] = jnp.zeros((256, TILE), jnp.bfloat16)

    for group, q_ref in enumerate((qa_ref, qb_ref)):

        def body(i, carry, group=group, q_ref=q_ref):
            tile(i, q_ref, group, z if group == 0 else 3 - z)
            return carry

        lax.fori_loop(0, 6, body, 0)


def attend(qa, qb, k_all, ext, v_all):
    return pl.pallas_call(
        attend_kernel,
        grid=(4,),
        in_specs=[
            pl.BlockSpec((4, 256, HALF), lambda kb: (0, 0, 0)),
            pl.BlockSpec((4, 256, HALF), lambda kb: (0, 0, 0)),
            pl.BlockSpec((1, BLOCK, 256), lambda kb: (kb, 0, 0)),
            pl.BlockSpec((1, BLOCK, 128), lambda kb: (kb, 0, 0)),
            pl.BlockSpec((1, 256, BLOCK), lambda kb: (kb, 0, 0)),
        ],
        out_specs=[
            pl.BlockSpec((1, 256, 4 * BLOCK), lambda kb: (kb, 0, 0)),
            pl.BlockSpec((16, 4 * BLOCK), lambda kb: (0, 0)),
        ],
        out_shape=[
            jax.ShapeDtypeStruct((4, 256, 4 * BLOCK), jnp.bfloat16),
            jax.ShapeDtypeStruct((16, 4 * BLOCK), jnp.float32),
        ],
        scratch_shapes=[
            pltpu.VMEM((BLOCK, TILE), jnp.float32),
            pltpu.VMEM((3, 256, TILE), jnp.bfloat16),
        ],
        compiler_params=pltpu.CompilerParams(
            dimension_semantics=("arbitrary",), vmem_limit_bytes=VMEM_LIMIT
        ),
        cost_estimate=pl.CostEstimate(
            flops=100_000_000_000, bytes_accessed=12_000_000, transcendentals=130_000_000
        ),
        name="attend",
    )(qa, qb, k_all, ext, v_all)


def sum_scratch(shape):
    bf16 = jnp.bfloat16
    return [
        pltpu.VMEM((4, *shape), bf16),
        pltpu.VMEM((4, *shape), bf16),
        pltpu.VMEM((2, shape[0] // 2, shape[1]), bf16),
        pltpu.VMEM((2, *shape), bf16),
    ]


def tp_sum(terms, collective_id, name):
    shape = (96, terms.shape[-1])
    return comm_call(
        tp_sum_kernel,
        [(shape, jnp.float32, vmem())],
        sum_scratch(shape),
        10,
        collective_id,
        name,
        [(terms.reshape(4, 2, *shape), vmem())],
    )[0]


def feed_kernel(
    rows, g1, gg, u1, uu, d1, dd1, d2, dd2, out, r_vmem, gate_w, up_w, down_w, gate, hidden, sems
):
    z, x = sp_coords()
    half = d1.shape[1]
    row_copy = pltpu.make_async_copy(rows, r_vmem, sems.at[64])
    row_copy.start()
    waits = [[], [], []]

    def fetch(stage, mine, own, other, dst, n):
        kept = pltpu.make_async_copy(own, dst, sems.at[n])
        came = pltpu.make_async_copy(other, dst, sems.at[n])
        pl.when(mine)(kept.start)
        pl.when(jnp.logical_not(mine))(came.start)
        waits[stage].append(came)

    spots = [(zp, xp, pl.ds((zp * 4 + xp) * 128, 128)) for zp in range(4) for xp in range(4)]
    for n, (zp, xp, lanes) in enumerate(spots):
        fetch(0, z == zp, g1.at[xp], gg.at[zp, xp], gate_w.at[:, lanes], n)
    for n, (zp, xp, lanes) in enumerate(spots):
        fetch(1, x == xp, u1.at[zp], uu.at[xp, zp], up_w.at[:, lanes], 16 + n)
    for n, (zp, xp, lanes) in enumerate(spots):
        fetch(2, z == zp, d1.at[xp], dd1.at[zp, xp], down_w.at[pl.ds(0, half), lanes], 32 + n)
        fetch(2, x == xp, d2.at[zp], dd2.at[xp, zp], down_w.at[pl.ds(half, half), lanes], 48 + n)
    turned = (((1,), (1,)), ((), ()))

    def over_rows(step):
        lax.fori_loop(0, 3, lambda i, c: (step(pl.ds(pl.multiple_of(i * 256, 256), 256)), c)[1], 0)

    row_copy.wait()
    for copy in waits[0]:
        copy.wait()

    def gates(span):
        gate[span, :] = lax.dot_general(
            r_vmem[span, :], gate_w[...], turned, preferred_element_type=jnp.float32
        )

    over_rows(gates)
    for copy in waits[1]:
        copy.wait()

    def hide(span):
        upper = lax.dot_general(
            r_vmem[span, :], up_w[...], turned, preferred_element_type=jnp.float32
        )
        value = gate[span, :]
        hidden[span, :] = (value / (1.0 + jnp.exp(-value)) * upper).astype(jnp.bfloat16)

    over_rows(hide)
    for copy in waits[2]:
        copy.wait()

    def lower(span):
        out[span, :] = jnp.dot(
            hidden[span, :], down_w[...], preferred_element_type=jnp.float32
        ).astype(jnp.bfloat16)

    over_rows(lower)


def feed(rows, *weights):
    units = weights[0].shape[1]
    bf16 = jnp.bfloat16
    return pl.pallas_call(
        feed_kernel,
        out_shape=jax.ShapeDtypeStruct((BLOCK, 2048), bf16),
        in_specs=[hbm()] * (1 + len(weights)),
        out_specs=vmem(),
        scratch_shapes=[
            pltpu.VMEM((BLOCK, 2048), bf16),
            pltpu.VMEM((units, 2048), bf16),
            pltpu.VMEM((units, 2048), bf16),
            pltpu.VMEM((units, 2048), bf16),
            pltpu.VMEM((BLOCK, units), jnp.float32),
            pltpu.VMEM((BLOCK, units), bf16),
            pltpu.SemaphoreType.DMA((65,)),
        ],
        compiler_params=pltpu.CompilerParams(vmem_limit_bytes=VMEM_LIMIT),
        cost_estimate=pl.CostEstimate(
            flops=6 * BLOCK * 2048 * units, bytes_accessed=15_000_000, transcendentals=BLOCK * units
        ),
        name="feed",
    )(rows, *weights)


def rounded(value):
    return lax.optimization_barrier(value.astype(jnp.bfloat16)).astype(jnp.float32)


def striped(value):
    return value.reshape(STRIPES, STRIPE, -1).swapaxes(0, 1).reshape(BLOCK, -1)


def on_device(
    query_small, key_small, value_small, offset_small, query_large, key_large, value_large, offset_large,
    out_small, out_large, residual, norm_gain, gate_weight, up_weight, down_weight,
):
    f32, bf16 = jnp.float32, jnp.bfloat16
    scales = np.concatenate(
        [np.full(128, LOG2E * SMALL_DIM**-0.5), np.full(128, LOG2E * LARGE_DIM**-0.5)]
    ).astype(np.float32)
    query = jnp.concatenate([query_small, query_large], axis=1).astype(f32) * scales
    query = query.astype(bf16).T
    key = striped(jnp.concatenate([key_small, key_large], axis=1))
    value = striped(jnp.concatenate([value_small, value_large], axis=1)).T
    offsets = jnp.concatenate([offset_small, offset_large], axis=0)
    offsets = offsets.reshape(3, STRIPES, STRIPE).swapaxes(1, 2).reshape(3, BLOCK)
    offsets = jnp.pad(offsets, ((0, 29), (0, 0)))
    gate, up, down = gate_weight.T, up_weight.T, down_weight
    units = down.shape[0]
    qa_all, qb_all, k_all, v_all, off_all, g1, d1 = comm_call(
        gather_kernel,
        [
            ((4, 256, HALF), bf16, vmem()),
            ((4, 256, HALF), bf16, vmem()),
            ((4, BLOCK, 256), bf16, vmem()),
            ((4, 256, BLOCK), bf16, vmem()),
            ((4, 32, BLOCK), bf16, vmem()),
            ((4, units, 128), bf16, hbm()),
            ((4, units // 2, 128), bf16, hbm()),
        ],
        [pltpu.VMEM((256, HALF), bf16), pltpu.SemaphoreType.DMA((2,))],
        43,
        0,
        "gather_qkv",
        [(array, vmem()) for array in (query[:, :HALF], query[:, HALF:], key, value, offsets, gate, down)],
    )
    spread = np.zeros((32, 128), np.float32)
    for head in range(3):
        spread[head, 3 * head : 3 * head + 3] = 1
    ext = jnp.einsum(
        "bhs,hc->bsc", off_all, jnp.asarray(spread, bf16), preferred_element_type=f32
    ).astype(bf16)
    outs, totals = attend(qa_all, qb_all, k_all, ext, v_all)
    half = (256, HALF)
    buffers = [pltpu.VMEM((4, 16, 4 * BLOCK), f32), pltpu.VMEM((4, 256, 4 * BLOCK), bf16)]
    for shape in ((4, *half), (2, 128, HALF), (2, *half), half):
        buffers += [pltpu.VMEM(shape, bf16)] * 2
    mixed, u1, d2 = comm_call(
        mix_kernel,
        [
            ((2, *half), bf16, vmem()),
            ((4, units, 128), bf16, hbm()),
            ((4, units // 2, 128), bf16, hbm()),
        ],
        [*buffers, pltpu.SemaphoreType.DMA((2,)), pltpu.SemaphoreType.DMA((8,))],
        31,
        1,
        "mix",
        [(totals, vmem()), (up, vmem()), (down, vmem()), (outs, hbm())],
    )
    out_weight = jnp.concatenate([out_small, out_large], axis=0)
    part = jnp.einsum("hct,cd->htd", mixed, out_weight, preferred_element_type=f32)
    shape = (96, part.shape[-1])
    terms = part.astype(bf16).reshape(4, 2, *shape)
    stream, rows, dd1, dd2, gg, uu = comm_call(
        middle_kernel,
        [
            (shape, f32, vmem()),
            ((4, 2, *shape), bf16, vmem()),
            ((4, *d1.shape), bf16, hbm()),
            ((4, *d2.shape), bf16, hbm()),
            ((4, *g1.shape), bf16, hbm()),
            ((4, *u1.shape), bf16, hbm()),
        ],
        [*sum_scratch(shape), pltpu.VMEM(shape, bf16)],
        47,
        3,
        "middle",
        [(terms, vmem()), (residual, vmem()), (norm_gain.reshape(1, -1), vmem())]
        + [(array, hbm()) for array in (d1, d2, g1, u1)],
    )
    down_terms = feed(rows.reshape(BLOCK, 2048), g1, gg, u1, uu, d1, dd1, d2, dd2)
    summed = tp_sum(down_terms, 5, "sum_tp_down")
    return (stream + rounded(summed)).astype(bf16)


def solution(mesh):
    return jax.shard_map(
        on_device,
        mesh=mesh,
        in_specs=(
            P("sp", "tp"), P("sp", "tp"), P("sp", "tp"), P("tp", "sp"),
            P("sp", "tp"), P("sp", "tp"), P("sp", "tp"), P("tp", "sp"),
            P("tp", None), P("tp", None), P(("sp", "tp"), None), P(),
            P("sp", "tp"), P("sp", "tp"), P("tp", "sp"),
        ),
        out_specs=P(("sp", "tp"), None),
        check_vma=False,
    )
```

```python
import functools
import math

import jax
import jax.numpy as jnp
import numpy as np
from jax import lax
from jax.experimental import pallas as pl
from jax.experimental.pallas import tpu as pltpu
from jax.sharding import PartitionSpec as P

SMALL_DIM = 64
LARGE_DIM = 128
BLOCK = 768
STRIPES = 8
STRIPE = BLOCK // STRIPES
TILE = 256
HALF = BLOCK // 2
LOG2E = math.log2(math.e)
MESH = pl.DeviceIdType.MESH
VMEM_LIMIT = 60 * 1024 * 1024


def vmem():
    return pl.BlockSpec(memory_space=pltpu.VMEM)


def sp_coords():
    index = lax.axis_index("sp")
    return index // 4, index % 4


def z_neighbours():
    z, x = sp_coords()
    return {"sp": ((z + 1) % 4) * 4 + x}, {"sp": ((z + 3) % 4) * 4 + x}


def x_neighbours():
    z, x = sp_coords()
    return {"sp": z * 4 + (x + 1) % 4}, {"sp": z * 4 + (x + 3) % 4}


def mirror():
    z, x = sp_coords()
    return {"sp": (3 - z) * 4 + x}


def y_neighbours():
    t = lax.axis_index("tp")
    return {"tp": (t + 2) % 8}, {"tp": (t + 6) % 8}


def sibling():
    t = lax.axis_index("tp")
    return {"tp": t + 1 - 2 * (t % 2)}


def greet(devices):
    barrier = pltpu.get_barrier_semaphore()
    for device in devices:
        pl.semaphore_signal(barrier, inc=1, device_id=device, device_id_type=MESH)
    pl.semaphore_wait(barrier, len(devices))


class Copies:
    def __init__(self, send_sems, recv_sems):
        self.send_sems, self.recv_sems, self.used, self.all = send_sems, recv_sems, 0, []

    def make(self, src, dst, device):
        k = self.used
        self.used += 1
        copy = pltpu.make_async_remote_copy(
            src_ref=src,
            dst_ref=dst,
            send_sem=self.send_sems.at[k],
            recv_sem=self.recv_sems.at[k],
            device_id=device,
            device_id_type=MESH,
        )
        self.all.append(copy)
        return copy

    def drain_sends(self):
        for copy in self.all:
            copy.wait_send()


def hbm():
    return pl.BlockSpec(memory_space=pl.ANY)


def comm_call(kernel, outs, scratch, copies, collective_id, name, args):
    return pl.pallas_call(
        kernel,
        out_shape=[jax.ShapeDtypeStruct(shape, dtype) for shape, dtype, _ in outs],
        in_specs=[spec for _, spec in args],
        out_specs=[spec for _, _, spec in outs],
        scratch_shapes=[
            *scratch,
            pltpu.SemaphoreType.DMA((copies,)),
            pltpu.SemaphoreType.DMA((copies,)),
        ],
        compiler_params=pltpu.CompilerParams(
            collective_id=collective_id, has_side_effects=True, vmem_limit_bytes=VMEM_LIMIT
        ),
        name=name,
    )(*(array for array, _ in args))


def by_rows(ref, part):
    half = ref.shape[-2] // 2
    return ref.at[(slice(None),) * (len(ref.shape) - 2) + (pl.ds(part * half, half),)]


def by_units(ref, part):
    half = ref.shape[0] // 2
    return ref.at[pl.ds(part * half, half)]


class RingGather:
    def __init__(self, copies, own, whole, me, ring, cut=by_rows):
        self.copies, self.own, self.whole, self.me, self.ring, self.cut = copies, own, whole, me, ring, cut

    def slot(self, place, part):
        return self.cut(self.whole.at[place], part)

    def start(self):
        right, left = self.ring
        self.sent = []
        for part, device in ((0, right), (1, left), (1, right), (0, left)):
            copy = self.copies.make(self.cut(self.own, part), self.slot(self.me, part), device)
            copy.start()
            self.sent.append(copy)

    def pass_on(self):
        right, left = self.ring
        for n, (place, device) in enumerate((((self.me + 3) % 4, right), ((self.me + 1) % 4, left))):
            self.sent[n].wait_recv()
            block = self.slot(place, n)
            copy = self.copies.make(block, block, device)
            copy.start()
            self.sent.append(copy)

    def finish(self):
        for copy in self.sent[2:]:
            copy.wait_recv()


class Keep:
    def __init__(self, sems):
        self.sems, self.all = sems, []

    def start(self, src, dst):
        copy = pltpu.make_async_copy(src, dst, self.sems.at[len(self.all)])
        copy.start()
        self.all.append(copy)

    def finish(self):
        for copy in self.all:
            copy.wait()


def gather_kernel(
    q_own, q_give, k, v, off, gate, down, qa_all, qb_all, k_all, v_all, off_all, g1, d1, q_got, keep_sems,
    send_sems, recv_sems,
):
    z, x = sp_coords()
    zs, xs = z_neighbours(), x_neighbours()
    greet((*zs, *xs))
    copies, keep = Copies(send_sems, recv_sems), Keep(keep_sems)
    swap = copies.make(q_give, q_got, mirror())
    swap.start()
    first = down.at[pl.ds(0, down.shape[0] // 2)]
    jobs = [
        RingGather(copies, k, k_all, z, zs),
        RingGather(copies, v, v_all, z, zs),
        RingGather(copies, off, off_all, z, zs),
        RingGather(copies, q_own, qa_all, x, xs),
        RingGather(copies, q_got, qb_all, x, xs),
        RingGather(copies, gate, g1, x, xs),
        RingGather(copies, first, d1, x, xs),
    ]
    for n, job in enumerate(jobs):
        if n == 4:
            swap.wait_recv()
        job.start()
    keep.start(gate, g1.at[x])
    keep.start(first, d1.at[x])
    for own, whole, me in ((k, k_all, z), (v, v_all, z), (off, off_all, z), (q_own, qa_all, x), (q_got, qb_all, x)):
        whole[me] = own[...]
    for job in jobs:
        job.pass_on()
    for job in jobs:
        job.finish()
    keep.finish()
    copies.drain_sends()


def plus(a, b):
    return (a.astype(jnp.float32) + b.astype(jnp.float32)).astype(jnp.bfloat16)


class RingSum:
    def __init__(self, copies, parts, relay, arrived, me, right, left, rows):
        half = rows // 2
        self.copies, self.parts, self.relay, self.arrived = copies, parts, relay, arrived
        self.me, self.right, self.left = me, right, left
        self.top, self.low = pl.ds(0, half), pl.ds(half, half)
        self.far, self.after, self.before = (me + 2) % 4, (me + 1) % 4, (me + 3) % 4
        self.waits = []

    def send(self, src, dst, device):
        copy = self.copies.make(src, dst, device)
        copy.start()
        return copy

    def send_far(self):
        self.a = self.send(self.parts.at[self.far, self.top], self.relay.at[0], self.right)
        self.b = self.send(self.parts.at[self.far, self.low], self.relay.at[1], self.left)

    def send_after(self):
        self.waits.append(
            self.send(self.parts.at[self.after, self.low], self.arrived.at[0, self.low], self.right)
        )

    def send_before(self):
        self.waits.append(
            self.send(self.parts.at[self.before, self.top], self.arrived.at[1, self.top], self.left)
        )

    def pass_on(self):
        self.a.wait_recv()
        self.parts[self.after, self.top] = plus(self.parts[self.after, self.top], self.relay[0])
        self.waits.append(
            self.send(self.parts.at[self.after, self.top], self.arrived.at[0, self.top], self.right)
        )
        self.b.wait_recv()
        self.parts[self.before, self.low] = plus(self.parts[self.before, self.low], self.relay[1])
        self.waits.append(
            self.send(self.parts.at[self.before, self.low], self.arrived.at[1, self.low], self.left)
        )

    def finish(self, own):
        for copy in self.waits:
            copy.wait_recv()
        return own + self.arrived[0].astype(jnp.float32) + self.arrived[1].astype(jnp.float32)


def scaled(o_ref, tot_ref, x, columns):
    nearer = jnp.zeros((4, HALF), jnp.float32)
    factors = [None] * 4
    for kb in reversed(range(4)):
        here = jnp.zeros((4, HALF), jnp.float32)
        block = jnp.zeros((4, HALF), jnp.float32)
        for other in range(4):
            term = tot_ref[other, kb * 4 : kb * 4 + 4, columns]
            block = block + term
            here = here + jnp.where(other > x, term, 0.0)
        factors[kb] = jnp.exp2(-(nearer + here))
        nearer = nearer + block
    pieces = []
    for head, _, row, size in HEADS:
        total = jnp.zeros((size, HALF), jnp.float32)
        for kb in range(4):
            term = o_ref[kb, row : row + size, columns].astype(jnp.float32)
            total = total + term * factors[kb][head : head + 1]
        pieces.append(total)
    return jnp.concatenate(pieces, axis=0)


def mix_kernel(
    tot, up, down, o_hbm, out, u1, d2, tot_all, o_ref, pa, pb, relay_a, relay_b, arrived_a, arrived_b, give, got,
    keep_sems, load_sems, send_sems, recv_sems,
):
    z, x = sp_coords()
    zs, xs = z_neighbours(), x_neighbours()
    greet((*zs, *xs))
    copies, keep = Copies(send_sems, recv_sems), Keep(keep_sems)
    second = down.at[pl.ds(down.shape[0] // 2, down.shape[0] // 2)]
    totals = RingGather(copies, tot, tot_all, x, xs)
    weights = [RingGather(copies, up, u1, z, zs), RingGather(copies, second, d2, z, zs)]
    totals.start()
    for job in weights:
        job.start()
    keep.start(up, u1.at[z])
    keep.start(second, d2.at[z])
    rings = [
        RingSum(copies, parts, relay, arrived, x, *xs, 256)
        for parts, relay, arrived in ((pb, relay_b, arrived_b), (pa, relay_a, arrived_a))
    ]

    def columns(group, place):
        return pl.ds(pl.multiple_of((group * 4 + place) * HALF, 128), HALF)

    loads = {}
    for n, (ring, group) in enumerate(zip(rings, (1, 0))):
        for m, place in enumerate((ring.far, ring.after, ring.before, x)):
            span = columns(group, place)
            loads[n, m] = pltpu.make_async_copy(
                o_hbm.at[:, :, span], o_ref.at[:, :, span], load_sems.at[n * 4 + m]
            )
            loads[n, m].start()
    tot_all[x] = tot[...]
    totals.pass_on()
    totals.finish()
    for n, (ring, group) in enumerate(zip(rings, (1, 0))):
        sends = (ring.send_far, ring.send_after, ring.send_before)
        for m, (place, send) in enumerate(zip((ring.far, ring.after, ring.before), sends)):
            loads[n, m].wait()
            ring.parts[place] = scaled(o_ref, tot_all, x, columns(group, place)).astype(jnp.bfloat16)
            send()
    for job in weights:
        job.pass_on()
    for ring in rings:
        ring.pass_on()
    loads[0, 3].wait()
    give[...] = rings[0].finish(scaled(o_ref, tot_all, x, columns(1, x))).astype(jnp.bfloat16)
    swap = copies.make(give, got, mirror())
    swap.start()
    loads[1, 3].wait()
    out[0] = rings[1].finish(scaled(o_ref, tot_all, x, columns(0, x))).astype(jnp.bfloat16)
    for job in weights:
        job.finish()
    keep.finish()
    swap.wait_recv()
    out[1] = got[...]
    copies.drain_sends()


def pair_sum(copies, terms, other, ring, y, core, mate):
    order = (ring.far, ring.after, ring.before, y)
    given = []
    for place in order:
        copy = copies.make(terms.at[place, 1 - core], other.at[place], mate)
        copy.start()
        given.append(copy)
    for place, copy, then in zip(order, given, (ring.send_far, ring.send_after, ring.send_before)):
        copy.wait_recv()
        ring.parts[place] = plus(terms[place, core], other[place])
        then()
    ring.pass_on()
    given[3].wait_recv()
    return terms[y, core].astype(jnp.float32) + other[y].astype(jnp.float32)


def tp_place():
    t = lax.axis_index("tp")
    return t // 2, t % 2


def tp_sum_kernel(terms, stream, out, other, parts, relay, arrived, send_sems, recv_sems):
    y, core = tp_place()
    ys, mate = y_neighbours(), sibling()
    greet((*ys, mate))
    copies = Copies(send_sems, recv_sems)
    ring = RingSum(copies, parts, relay, arrived, y, *ys, 96)
    own = pair_sum(copies, terms, other, ring, y, core, mate)
    summed = ring.finish(own).astype(jnp.bfloat16).astype(jnp.float32)
    out[...] = (stream[...] + summed).astype(jnp.bfloat16)
    copies.drain_sends()


def middle_kernel(
    mixed, out_small, out_large, residual, gain, d1, d2, g1, u1, stream, whole, dd1, dd2, gg, uu, other, parts,
    relay, arrived, own, terms, send_sems, recv_sems,
):
    z, x = sp_coords()
    y, core = tp_place()
    zs, xs, ys, mate = z_neighbours(), x_neighbours(), y_neighbours(), sibling()
    greet((*ys, mate, *zs, *xs))
    copies = Copies(send_sems, recv_sems)
    early = [
        RingGather(copies, d2, dd2, x, xs, by_units),
        RingGather(copies, d1, dd1, z, zs, by_units),
    ]
    late = [
        RingGather(copies, u1, uu, x, xs, by_units),
        RingGather(copies, g1, gg, z, zs, by_units),
    ]
    ring = RingSum(copies, parts, relay, arrived, y, *ys, 96)
    for job in early + late:
        job.start()
    turned = (((0,), (0,)), ((), ()))
    for n in range(2):
        part = lax.dot_general(
            mixed[n, 0:128], out_small[...], turned, preferred_element_type=jnp.float32
        ) + lax.dot_general(mixed[n, 128:256], out_large[...], turned, preferred_element_type=jnp.float32)
        terms[2 * n : 2 * n + 2] = part.astype(jnp.bfloat16).reshape(2, 2, *residual.shape)
    total = pair_sum(copies, terms, other, ring, y, core, mate)
    for job in early:
        job.pass_on()
    attended = ring.finish(total).astype(jnp.bfloat16).astype(jnp.float32)
    value = residual[...].astype(jnp.float32) + attended
    stream[...] = value
    scale = lax.rsqrt(jnp.mean(value * value, axis=-1, keepdims=True) + 1e-06)
    own[...] = (value * scale * gain[...].astype(jnp.float32)).astype(jnp.bfloat16)

    right, left = ys
    before, after, far = (y + 3) % 4, (y + 1) % 4, (y + 2) % 4
    top, low = pl.ds(0, 48), pl.ds(48, 48)
    sent = (
        copies.make(own.at[top], whole.at[y, core, top], right),
        copies.make(own.at[low], whole.at[y, core, low], left),
        copies.make(own.at[low], whole.at[y, core, low], right),
        copies.make(own.at[top], whole.at[y, core, top], left),
        copies.make(own, whole.at[y, core], mate),
    )
    for copy in sent:
        copy.start()
    whole[y, core] = own[...]
    over = [sent[4]]

    def send(block, device):
        copy = copies.make(block, block, device)
        copy.start()
        return copy

    sent[0].wait_recv()
    on_right = send(whole.at[before, core, top], right)
    over.append(send(whole.at[before, core, top], mate))
    sent[1].wait_recv()
    on_left = send(whole.at[after, core, low], left)
    over.append(send(whole.at[after, core, low], mate))
    for job in late:
        job.pass_on()
    sent[2].wait_recv()
    over.append(send(whole.at[before, core, low], mate))
    sent[3].wait_recv()
    over.append(send(whole.at[after, core, top], mate))
    on_right.wait_recv()
    over.append(send(whole.at[far, core, top], mate))
    on_left.wait_recv()
    over.append(send(whole.at[far, core, low], mate))
    for copy in over:
        copy.wait_recv()
    for job in early + late:
        job.finish()
    copies.drain_sends()


HEADS = ((0, 0, 0, 64), (1, 0, 64, 64), (2, 128, 128, 128))


def selector(head):
    rows = lax.broadcasted_iota(jnp.int32, (128, TILE), 0)
    pieces, rest = [], LOG2E
    for _ in range(3):
        piece = float(np.asarray(rest, dtype=jnp.bfloat16.dtype).astype(np.float64))
        pieces.append(piece)
        rest -= piece
    value = jnp.zeros((128, TILE), jnp.float32)
    for n, piece in enumerate(pieces):
        value = jnp.where(rows == 3 * head + n, piece, value)
    return value.astype(jnp.bfloat16)


def attend_kernel(
    qa_ref, qb_ref, k_ref, off_ref, spread_ref, v_ref, o_ref, tot_ref, work_ref, rhs_ref, ext_ref,
    wide_ref,
):
    z, x = sp_coords()
    kb = pl.program_id(0)

    wide_ref[...] = lax.dot_general(
        off_ref[0], spread_ref[...], (((0,), (0,)), ((), ())), preferred_element_type=jnp.float32
    )
    for j in range(0, STRIPE, 2):
        pair = [eight_keys(wide_ref, j), eight_keys(wide_ref, j + 1)]
        ext_ref[j * 8 : j * 8 + 16, :] = jnp.concatenate(pair, axis=0).astype(jnp.bfloat16)

    @pl.when(kb == 0)
    def _():
        tot_ref[...] = jnp.zeros_like(tot_ref)
        for head, key_column, row, rows in HEADS:
            rhs_ref[head, 128:256, :] = selector(head)
            if rows == 64:
                rhs_ref[head, 64 - row : 128 - row, :] = jnp.zeros((64, TILE), jnp.bfloat16)

    def tile(i, q_ref, group, own_z):
        first = pl.multiple_of(i * TILE, TILE)
        columns = pl.ds(pl.multiple_of(group * 2 * BLOCK + i * TILE, TILE), TILE)

        def run(masked):
            for head, key_column, row, rows in HEADS:
                inner = row if rows == 64 else 0
                for n in range(2):
                    piece = 2 * i + n
                    rhs_ref[head, inner : inner + rows, n * 128 : (n + 1) * 128] = q_ref[
                        piece // 3, row : row + rows, pl.ds(pl.multiple_of(piece % 3 * 128, 128), 128)
                    ]
                rhs = rhs_ref[head]
                sums = jnp.zeros((8, TILE), jnp.float32)
                chunk = 128
                if masked:
                    query = lax.broadcasted_iota(jnp.int32, (1, TILE), 1) + first
                    query_pos = query + (query // HALF - x * 2 + group) * HALF
                for c in reversed(range(BLOCK // chunk)):
                    span = slice(c * chunk, (c + 1) * chunk)
                    lhs = jnp.concatenate(
                        [k_ref[0, span, key_column : key_column + 128], ext_ref[span, :]], axis=1
                    )
                    logit = jnp.dot(lhs, rhs, preferred_element_type=jnp.float32)
                    loss = jnp.maximum(
                        logit, jnp.log2(1.0 + jnp.exp2(jnp.minimum(logit, 100.0)))
                    )
                    if masked:
                        at = lax.broadcasted_iota(jnp.int32, (chunk, TILE), 0) + c * chunk
                        key_pos = (at % 8) * STRIPE + at // 8
                        live = key_pos < query_pos
                        loss = jnp.where(live, loss, 0.0)
                        logit = jnp.where(live, logit, -1e30)
                    for j in reversed(range(chunk // 8)):
                        eight = slice(j * 8, (j + 1) * 8)
                        sums = sums + loss[eight]
                        work_ref[c * chunk + j * 8 : c * chunk + (j + 1) * 8, :] = logit[eight] - sums
                later = [jnp.zeros((1, TILE), jnp.float32)]
                for r in range(7, 0, -1):
                    later.append(later[-1] + sums[r : r + 1])
                tot_ref[pl.ds(kb * 4 + head, 1), columns] = later[-1] + sums[0:1]
                behind = jnp.concatenate(later[::-1], axis=0)
                total = jnp.zeros((rows, TILE), jnp.float32)
                for c in range(BLOCK // 256):
                    span = slice(c * 256, (c + 1) * 256)
                    power = work_ref[span, :].reshape(32, 8, TILE) - behind[None]
                    weight = jnp.exp2(power).reshape(256, TILE).astype(jnp.bfloat16)
                    total = total + jnp.dot(
                        v_ref[0, row : row + rows, span], weight, preferred_element_type=jnp.float32
                    )
                o_ref[0, row : row + rows, columns] = total.astype(jnp.bfloat16)

        place, last = first // HALF, (first + TILE - 1) // HALF
        whole = jnp.logical_or(kb < own_z, jnp.logical_and(kb == own_z, place > x))
        none = jnp.logical_or(kb > own_z, jnp.logical_and(kb == own_z, last < x))
        partly = jnp.logical_not(jnp.logical_or(whole, none))

        @pl.when(whole)
        def _():
            run(False)

        @pl.when(partly)
        def _():
            run(True)

        @pl.when(none)
        def _():
            o_ref[0, :, columns] = jnp.zeros((256, TILE), jnp.bfloat16)

    for group, q_ref in enumerate((qa_ref, qb_ref)):

        def body(i, carry, group=group, q_ref=q_ref):
            tile(i, q_ref, group, z if group == 0 else 3 - z)
            return carry

        lax.fori_loop(0, 6, body, 0)


def attend(qa, qb, k_all, off_all, spread, v_all):
    return pl.pallas_call(
        attend_kernel,
        grid=(4,),
        in_specs=[
            pl.BlockSpec((4, 256, HALF), lambda kb: (0, 0, 0)),
            pl.BlockSpec((4, 256, HALF), lambda kb: (0, 0, 0)),
            pl.BlockSpec((1, BLOCK, 256), lambda kb: (kb, 0, 0)),
            pl.BlockSpec((1, 32, BLOCK), lambda kb: (kb, 0, 0)),
            pl.BlockSpec((32, 128), lambda kb: (0, 0)),
            pl.BlockSpec((1, 256, BLOCK), lambda kb: (kb, 0, 0)),
        ],
        out_specs=[
            pl.BlockSpec((1, 256, 4 * BLOCK), lambda kb: (kb, 0, 0)),
            pl.BlockSpec((16, 4 * BLOCK), lambda kb: (0, 0)),
        ],
        out_shape=[
            jax.ShapeDtypeStruct((4, 256, 4 * BLOCK), jnp.bfloat16),
            jax.ShapeDtypeStruct((16, 4 * BLOCK), jnp.float32),
        ],
        scratch_shapes=[
            pltpu.VMEM((BLOCK, TILE), jnp.float32),
            pltpu.VMEM((3, 256, TILE), jnp.bfloat16),
            pltpu.VMEM((BLOCK, 128), jnp.bfloat16),
            pltpu.VMEM((BLOCK, 128), jnp.float32),
        ],
        compiler_params=pltpu.CompilerParams(
            dimension_semantics=("arbitrary",), vmem_limit_bytes=VMEM_LIMIT
        ),
        cost_estimate=pl.CostEstimate(
            flops=100_000_000_000, bytes_accessed=12_000_000, transcendentals=130_000_000
        ),
        name="attend",
    )(qa, qb, k_all, off_all, spread, v_all)


def sum_scratch(shape):
    bf16 = jnp.bfloat16
    return [
        pltpu.VMEM((4, *shape), bf16),
        pltpu.VMEM((4, *shape), bf16),
        pltpu.VMEM((2, shape[0] // 2, shape[1]), bf16),
        pltpu.VMEM((2, *shape), bf16),
    ]


def tp_sum(terms, stream, collective_id, name):
    shape = (96, terms.shape[-1])
    return comm_call(
        tp_sum_kernel,
        [(shape, jnp.bfloat16, vmem())],
        sum_scratch(shape),
        10,
        collective_id,
        name,
        [(terms.reshape(4, 2, *shape), vmem()), (stream, vmem())],
    )[0]


def feed_kernel(
    rows, g1, gg, u1, uu, d1, dd1, d2, dd2, out, r_vmem, gate_w, up_w, down_w, gate, hidden, sems
):
    z, x = sp_coords()
    half = d1.shape[1]
    row_copy = pltpu.make_async_copy(rows, r_vmem, sems.at[64])
    row_copy.start()
    waits = [[], [], []]

    def fetch(stage, mine, own, other, dst, n):
        kept = pltpu.make_async_copy(own, dst, sems.at[n])
        came = pltpu.make_async_copy(other, dst, sems.at[n])
        pl.when(mine)(kept.start)
        pl.when(jnp.logical_not(mine))(came.start)
        waits[stage].append(came)

    spots = [(zp, xp, pl.ds((zp * 4 + xp) * 128, 128)) for zp in range(4) for xp in range(4)]
    for n, (zp, xp, lanes) in enumerate(spots):
        fetch(0, z == zp, g1.at[xp], gg.at[zp, xp], gate_w.at[:, lanes], n)
    for n, (zp, xp, lanes) in enumerate(spots):
        fetch(1, x == xp, u1.at[zp], uu.at[xp, zp], up_w.at[:, lanes], 16 + n)
    for n, (zp, xp, lanes) in enumerate(spots):
        fetch(2, z == zp, d1.at[xp], dd1.at[zp, xp], down_w.at[pl.ds(0, half), lanes], 32 + n)
        fetch(2, x == xp, d2.at[zp], dd2.at[xp, zp], down_w.at[pl.ds(half, half), lanes], 48 + n)
    turned = (((1,), (1,)), ((), ()))

    def over_rows(step):
        lax.fori_loop(0, 3, lambda i, c: (step(pl.ds(pl.multiple_of(i * 256, 256), 256)), c)[1], 0)

    row_copy.wait()
    for copy in waits[0]:
        copy.wait()

    def gates(span):
        gate[span, :] = lax.dot_general(
            r_vmem[span, :], gate_w[...], turned, preferred_element_type=jnp.float32
        )

    over_rows(gates)
    for copy in waits[1]:
        copy.wait()

    def hide(span):
        upper = lax.dot_general(
            r_vmem[span, :], up_w[...], turned, preferred_element_type=jnp.float32
        )
        value = gate[span, :]
        hidden[span, :] = (value / (1.0 + jnp.exp(-value)) * upper).astype(jnp.bfloat16)

    over_rows(hide)
    for copy in waits[2]:
        copy.wait()

    def lower(span):
        out[span, :] = jnp.dot(
            hidden[span, :], down_w[...], preferred_element_type=jnp.float32
        ).astype(jnp.bfloat16)

    over_rows(lower)


def feed(rows, *weights):
    units = weights[0].shape[1]
    bf16 = jnp.bfloat16
    return pl.pallas_call(
        feed_kernel,
        out_shape=jax.ShapeDtypeStruct((BLOCK, 2048), bf16),
        in_specs=[hbm()] * (1 + len(weights)),
        out_specs=vmem(),
        scratch_shapes=[
            pltpu.VMEM((BLOCK, 2048), bf16),
            pltpu.VMEM((units, 2048), bf16),
            pltpu.VMEM((units, 2048), bf16),
            pltpu.VMEM((units, 2048), bf16),
            pltpu.VMEM((BLOCK, units), jnp.float32),
            pltpu.VMEM((BLOCK, units), bf16),
            pltpu.SemaphoreType.DMA((65,)),
        ],
        compiler_params=pltpu.CompilerParams(vmem_limit_bytes=VMEM_LIMIT),
        cost_estimate=pl.CostEstimate(
            flops=6 * BLOCK * 2048 * units, bytes_accessed=15_000_000, transcendentals=BLOCK * units
        ),
        name="feed",
    )(rows, *weights)


def eight_keys(ref, j):
    return ref[pl.ds(j, STRIPES, stride=STRIPE), :]


def prepare_kernel(qs, ks, vs, ql, kl, vl, q_own, q_give, key, value, wide, turned):
    f32, bf16 = jnp.float32, jnp.bfloat16
    for n, (q, depth) in enumerate(((qs, SMALL_DIM), (ql, LARGE_DIM))):
        rows = slice(n * 128, (n + 1) * 128)
        flipped = (q[...].astype(f32) * float(np.float32(LOG2E * depth**-0.5))).T.astype(bf16)
        q_own[rows, :] = flipped[:, :HALF]
        q_give[rows, :] = flipped[:, HALF:]
    for n, (k, v) in enumerate(((ks, vs), (kl, vl))):
        columns = slice(n * 128, (n + 1) * 128)
        wide[2 * n] = k[...].astype(f32)
        wide[2 * n + 1] = v[...].astype(f32)
        for j in range(0, STRIPE, 2):
            pair = [eight_keys(wide.at[2 * n], j), eight_keys(wide.at[2 * n], j + 1)]
            key[j * 8 : j * 8 + 16, columns] = jnp.concatenate(pair, axis=0).astype(bf16)
            for i in (j, j + 1):
                turned[n, i * 8 : i * 8 + 8, :] = eight_keys(wide.at[2 * n + 1], i)
        value[columns, :] = turned[n].T.astype(bf16)


def prepare(*arrays):
    bf16 = jnp.bfloat16
    shapes = ((256, HALF), (256, HALF), (BLOCK, 256), (256, BLOCK))
    return pl.pallas_call(
        prepare_kernel,
        out_shape=[jax.ShapeDtypeStruct(shape, bf16) for shape in shapes],
        in_specs=[vmem()] * 6,
        out_specs=[vmem()] * 4,
        scratch_shapes=[
            pltpu.VMEM((4, BLOCK, 128), jnp.float32),
            pltpu.VMEM((2, BLOCK, 128), jnp.float32),
        ],
        name="prepare",
    )(*arrays)


def on_device(
    query_small, key_small, value_small, offset_small, query_large, key_large, value_large, offset_large,
    out_small, out_large, residual, norm_gain, gate_weight, up_weight, down_weight,
):
    f32, bf16 = jnp.float32, jnp.bfloat16
    q_own, q_give, key, value = prepare(
        query_small, key_small, value_small, query_large, key_large, value_large
    )
    offsets = jnp.concatenate([offset_small, offset_large], axis=0)
    offsets = jnp.pad(offsets, ((0, 29), (0, 0)))
    gate, up, down = gate_weight.T, up_weight.T, down_weight
    units = down.shape[0]
    qa_all, qb_all, k_all, v_all, off_all, g1, d1 = comm_call(
        gather_kernel,
        [
            ((4, 256, HALF), bf16, vmem()),
            ((4, 256, HALF), bf16, vmem()),
            ((4, BLOCK, 256), bf16, vmem()),
            ((4, 256, BLOCK), bf16, vmem()),
            ((4, 32, BLOCK), bf16, vmem()),
            ((4, units, 128), bf16, hbm()),
            ((4, units // 2, 128), bf16, hbm()),
        ],
        [pltpu.VMEM((256, HALF), bf16), pltpu.SemaphoreType.DMA((2,))],
        43,
        0,
        "gather_qkv",
        [(array, vmem()) for array in (q_own, q_give, key, value, offsets, gate, down)],
    )
    spread = np.zeros((32, 128), np.float32)
    for head in range(3):
        spread[head, 3 * head : 3 * head + 3] = 1
    outs, totals = attend(qa_all, qb_all, k_all, off_all, jnp.asarray(spread, bf16), v_all)
    half = (256, HALF)
    buffers = [pltpu.VMEM((4, 16, 4 * BLOCK), f32), pltpu.VMEM((4, 256, 4 * BLOCK), bf16)]
    for shape in ((4, *half), (2, 128, HALF), (2, *half), half):
        buffers += [pltpu.VMEM(shape, bf16)] * 2
    mixed, u1, d2 = comm_call(
        mix_kernel,
        [
            ((2, *half), bf16, vmem()),
            ((4, units, 128), bf16, hbm()),
            ((4, units // 2, 128), bf16, hbm()),
        ],
        [*buffers, pltpu.SemaphoreType.DMA((2,)), pltpu.SemaphoreType.DMA((8,))],
        31,
        1,
        "mix",
        [(totals, vmem()), (up, vmem()), (down, vmem()), (outs, hbm())],
    )
    shape = residual.shape
    stream, rows, dd1, dd2, gg, uu = comm_call(
        middle_kernel,
        [
            (shape, f32, vmem()),
            ((4, 2, *shape), bf16, vmem()),
            ((4, *d1.shape), bf16, hbm()),
            ((4, *d2.shape), bf16, hbm()),
            ((4, *g1.shape), bf16, hbm()),
            ((4, *u1.shape), bf16, hbm()),
        ],
        [*sum_scratch(shape), pltpu.VMEM(shape, bf16), pltpu.VMEM((4, 2, *shape), bf16)],
        47,
        3,
        "middle",
        [
            (array, vmem())
            for array in (mixed, out_small, out_large, residual, norm_gain.astype(f32).reshape(1, -1))
        ]
        + [(array, hbm()) for array in (d1, d2, g1, u1)],
    )
    down_terms = feed(rows.reshape(BLOCK, 2048), g1, gg, u1, uu, d1, dd1, d2, dd2)
    return tp_sum(down_terms, stream, 5, "sum_tp_down")


def solution(mesh):
    return jax.shard_map(
        on_device,
        mesh=mesh,
        in_specs=(
            P("sp", "tp"), P("sp", "tp"), P("sp", "tp"), P("tp", "sp"),
            P("sp", "tp"), P("sp", "tp"), P("sp", "tp"), P("tp", "sp"),
            P("tp", None), P("tp", None), P(("sp", "tp"), None), P(),
            P("sp", "tp"), P("sp", "tp"), P("tp", "sp"),
        ),
        out_specs=P(("sp", "tp"), None),
        check_vma=False,
    )
```

```python
import functools
import math

import jax
import jax.numpy as jnp
import numpy as np
from jax import lax
from jax.experimental import pallas as pl
from jax.experimental.pallas import tpu as pltpu
from jax.sharding import PartitionSpec as P

SMALL_DIM = 64
LARGE_DIM = 128
BLOCK = 768
STRIPES = 8
STRIPE = BLOCK // STRIPES
TILE = 256
HALF = BLOCK // 2
LOG2E = math.log2(math.e)
MESH = pl.DeviceIdType.MESH
VMEM_LIMIT = 60 * 1024 * 1024


def vmem():
    return pl.BlockSpec(memory_space=pltpu.VMEM)


def sp_coords():
    index = lax.axis_index("sp")
    return index // 4, index % 4


def z_neighbours():
    z, x = sp_coords()
    return {"sp": ((z + 1) % 4) * 4 + x}, {"sp": ((z + 3) % 4) * 4 + x}


def x_neighbours():
    z, x = sp_coords()
    return {"sp": z * 4 + (x + 1) % 4}, {"sp": z * 4 + (x + 3) % 4}


def mirror():
    z, x = sp_coords()
    return {"sp": (3 - z) * 4 + x}


def y_neighbours():
    t = lax.axis_index("tp")
    return {"tp": (t + 2) % 8}, {"tp": (t + 6) % 8}


def sibling():
    t = lax.axis_index("tp")
    return {"tp": t + 1 - 2 * (t % 2)}


def greet(devices):
    barrier = pltpu.get_barrier_semaphore()
    for device in devices:
        pl.semaphore_signal(barrier, inc=1, device_id=device, device_id_type=MESH)
    pl.semaphore_wait(barrier, len(devices))


class Copies:
    def __init__(self, send_sems, recv_sems):
        self.send_sems, self.recv_sems, self.used, self.all = send_sems, recv_sems, 0, []

    def make(self, src, dst, device):
        k = self.used
        self.used += 1
        copy = pltpu.make_async_remote_copy(
            src_ref=src,
            dst_ref=dst,
            send_sem=self.send_sems.at[k],
            recv_sem=self.recv_sems.at[k],
            device_id=device,
            device_id_type=MESH,
        )
        self.all.append(copy)
        return copy

    def drain_sends(self):
        for copy in self.all:
            copy.wait_send()


def hbm():
    return pl.BlockSpec(memory_space=pl.ANY)


def comm_call(kernel, outs, scratch, copies, collective_id, name, args):
    return pl.pallas_call(
        kernel,
        out_shape=[jax.ShapeDtypeStruct(shape, dtype) for shape, dtype, _ in outs],
        in_specs=[spec for _, spec in args],
        out_specs=[spec for _, _, spec in outs],
        scratch_shapes=[
            *scratch,
            pltpu.SemaphoreType.DMA((copies,)),
            pltpu.SemaphoreType.DMA((copies,)),
        ],
        compiler_params=pltpu.CompilerParams(
            collective_id=collective_id, has_side_effects=True, vmem_limit_bytes=VMEM_LIMIT
        ),
        name=name,
    )(*(array for array, _ in args))


def by_rows(ref, part):
    half = ref.shape[-2] // 2
    return ref.at[(slice(None),) * (len(ref.shape) - 2) + (pl.ds(part * half, half),)]


def by_units(ref, part):
    half = ref.shape[0] // 2
    return ref.at[pl.ds(part * half, half)]


class RingGather:
    def __init__(self, copies, own, whole, me, ring, cut=by_rows):
        self.copies, self.own, self.whole, self.me, self.ring, self.cut = copies, own, whole, me, ring, cut

    def slot(self, place, part):
        return self.cut(self.whole.at[place], part)

    def start(self):
        right, left = self.ring
        self.sent = []
        for part, device in ((0, right), (1, left), (1, right), (0, left)):
            copy = self.copies.make(self.cut(self.own, part), self.slot(self.me, part), device)
            copy.start()
            self.sent.append(copy)

    def pass_on(self):
        right, left = self.ring
        for n, (place, device) in enumerate((((self.me + 3) % 4, right), ((self.me + 1) % 4, left))):
            self.sent[n].wait_recv()
            block = self.slot(place, n)
            copy = self.copies.make(block, block, device)
            copy.start()
            self.sent.append(copy)

    def finish(self):
        for copy in self.sent[2:]:
            copy.wait_recv()


class Keep:
    def __init__(self, sems):
        self.sems, self.all = sems, []

    def start(self, src, dst):
        copy = pltpu.make_async_copy(src, dst, self.sems.at[len(self.all)])
        copy.start()
        self.all.append(copy)

    def finish(self):
        for copy in self.all:
            copy.wait()


def gather_kernel(
    q_own, q_give, k, v, off, gate, down, qa_all, qb_all, k_all, v_all, off_all, g1, d1, q_got, keep_sems,
    send_sems, recv_sems,
):
    z, x = sp_coords()
    zs, xs = z_neighbours(), x_neighbours()
    greet((*zs, *xs))
    copies, keep = Copies(send_sems, recv_sems), Keep(keep_sems)
    swap = copies.make(q_give, q_got, mirror())
    swap.start()
    first = down.at[pl.ds(0, down.shape[0] // 2)]
    jobs = [
        RingGather(copies, k, k_all, z, zs),
        RingGather(copies, v, v_all, z, zs),
        RingGather(copies, off, off_all, z, zs),
        RingGather(copies, q_own, qa_all, x, xs),
        RingGather(copies, q_got, qb_all, x, xs),
        RingGather(copies, gate, g1, x, xs),
        RingGather(copies, first, d1, x, xs),
    ]
    for n, job in enumerate(jobs):
        if n == 4:
            swap.wait_recv()
        job.start()
    keep.start(gate, g1.at[x])
    keep.start(first, d1.at[x])
    for own, whole, me in ((k, k_all, z), (v, v_all, z), (off, off_all, z), (q_own, qa_all, x), (q_got, qb_all, x)):
        whole[me] = own[...]
    for job in jobs:
        job.pass_on()
    for job in jobs:
        job.finish()
    keep.finish()
    copies.drain_sends()


def plus(a, b):
    return (a.astype(jnp.float32) + b.astype(jnp.float32)).astype(jnp.bfloat16)


class RingSum:
    def __init__(self, copies, parts, relay, arrived, me, right, left, rows):
        half = rows // 2
        self.copies, self.parts, self.relay, self.arrived = copies, parts, relay, arrived
        self.me, self.right, self.left = me, right, left
        self.top, self.low = pl.ds(0, half), pl.ds(half, half)
        self.far, self.after, self.before = (me + 2) % 4, (me + 1) % 4, (me + 3) % 4
        self.waits = []

    def send(self, src, dst, device):
        copy = self.copies.make(src, dst, device)
        copy.start()
        return copy

    def send_far(self):
        self.a = self.send(self.parts.at[self.far, self.top], self.relay.at[0], self.right)
        self.b = self.send(self.parts.at[self.far, self.low], self.relay.at[1], self.left)

    def send_after(self):
        self.waits.append(
            self.send(self.parts.at[self.after, self.low], self.arrived.at[0, self.low], self.right)
        )

    def send_before(self):
        self.waits.append(
            self.send(self.parts.at[self.before, self.top], self.arrived.at[1, self.top], self.left)
        )

    def pass_on(self):
        self.a.wait_recv()
        self.parts[self.after, self.top] = plus(self.parts[self.after, self.top], self.relay[0])
        self.waits.append(
            self.send(self.parts.at[self.after, self.top], self.arrived.at[0, self.top], self.right)
        )
        self.b.wait_recv()
        self.parts[self.before, self.low] = plus(self.parts[self.before, self.low], self.relay[1])
        self.waits.append(
            self.send(self.parts.at[self.before, self.low], self.arrived.at[1, self.low], self.left)
        )

    def finish(self, own):
        for copy in self.waits:
            copy.wait_recv()
        return own + self.arrived[0].astype(jnp.float32) + self.arrived[1].astype(jnp.float32)


def scaled(o_ref, tot_ref, x, columns):
    nearer = jnp.zeros((4, HALF), jnp.float32)
    factors = [None] * 4
    for kb in reversed(range(4)):
        here = jnp.zeros((4, HALF), jnp.float32)
        block = jnp.zeros((4, HALF), jnp.float32)
        for other in range(4):
            term = tot_ref[other, kb * 4 : kb * 4 + 4, columns]
            block = block + term
            here = here + jnp.where(other > x, term, 0.0)
        factors[kb] = jnp.exp2(-(nearer + here))
        nearer = nearer + block
    pieces = []
    for head, _, row, size in HEADS:
        total = jnp.zeros((size, HALF), jnp.float32)
        for kb in range(4):
            term = o_ref[kb, row : row + size, columns].astype(jnp.float32)
            total = total + term * factors[kb][head : head + 1]
        pieces.append(total)
    return jnp.concatenate(pieces, axis=0)


def mix_kernel(
    tot, up, down, o_hbm, out, u1, d2, tot_all, o_ref, pa, pb, relay_a, relay_b, arrived_a, arrived_b, give, got,
    keep_sems, load_sems, send_sems, recv_sems,
):
    z, x = sp_coords()
    zs, xs = z_neighbours(), x_neighbours()
    greet((*zs, *xs))
    copies, keep = Copies(send_sems, recv_sems), Keep(keep_sems)
    second = down.at[pl.ds(down.shape[0] // 2, down.shape[0] // 2)]
    totals = RingGather(copies, tot, tot_all, x, xs)
    weights = [RingGather(copies, up, u1, z, zs), RingGather(copies, second, d2, z, zs)]
    totals.start()
    for job in weights:
        job.start()
    keep.start(up, u1.at[z])
    keep.start(second, d2.at[z])
    rings = [
        RingSum(copies, parts, relay, arrived, x, *xs, 256)
        for parts, relay, arrived in ((pb, relay_b, arrived_b), (pa, relay_a, arrived_a))
    ]

    def columns(group, place):
        return pl.ds(pl.multiple_of((group * 4 + place) * HALF, 128), HALF)

    loads = {}
    for n, (ring, group) in enumerate(zip(rings, (1, 0))):
        for m, place in enumerate((ring.far, ring.after, ring.before, x)):
            span = columns(group, place)
            loads[n, m] = pltpu.make_async_copy(
                o_hbm.at[:, :, span], o_ref.at[:, :, span], load_sems.at[n * 4 + m]
            )
            loads[n, m].start()
    tot_all[x] = tot[...]
    totals.pass_on()
    totals.finish()
    for n, (ring, group) in enumerate(zip(rings, (1, 0))):
        sends = (ring.send_far, ring.send_after, ring.send_before)
        for m, (place, send) in enumerate(zip((ring.far, ring.after, ring.before), sends)):
            loads[n, m].wait()
            ring.parts[place] = scaled(o_ref, tot_all, x, columns(group, place)).astype(jnp.bfloat16)
            send()
    for job in weights:
        job.pass_on()
    for ring in rings:
        ring.pass_on()
    loads[0, 3].wait()
    give[...] = rings[0].finish(scaled(o_ref, tot_all, x, columns(1, x))).astype(jnp.bfloat16)
    swap = copies.make(give, got, mirror())
    swap.start()
    loads[1, 3].wait()
    out[0] = rings[1].finish(scaled(o_ref, tot_all, x, columns(0, x))).astype(jnp.bfloat16)
    for job in weights:
        job.finish()
    keep.finish()
    swap.wait_recv()
    out[1] = got[...]
    copies.drain_sends()


def pair_sum(copies, terms, other, ring, y, core, mate):
    order = (ring.far, ring.after, ring.before, y)
    given = []
    for place in order:
        copy = copies.make(terms.at[place, 1 - core], other.at[place], mate)
        copy.start()
        given.append(copy)
    for place, copy, then in zip(order, given, (ring.send_far, ring.send_after, ring.send_before)):
        copy.wait_recv()
        ring.parts[place] = plus(terms[place, core], other[place])
        then()
    ring.pass_on()
    given[3].wait_recv()
    return terms[y, core].astype(jnp.float32) + other[y].astype(jnp.float32)


def tp_place():
    t = lax.axis_index("tp")
    return t // 2, t % 2


def middle_kernel(
    mixed, out_small, out_large, residual, gain, d1, d2, g1, u1, stream, whole, dd1, dd2, gg, uu, other, parts,
    relay, arrived, own, terms, send_sems, recv_sems,
):
    z, x = sp_coords()
    y, core = tp_place()
    zs, xs, ys, mate = z_neighbours(), x_neighbours(), y_neighbours(), sibling()
    greet((*ys, mate, *zs, *xs))
    copies = Copies(send_sems, recv_sems)
    early = [
        RingGather(copies, d2, dd2, x, xs, by_units),
        RingGather(copies, d1, dd1, z, zs, by_units),
    ]
    late = [
        RingGather(copies, u1, uu, x, xs, by_units),
        RingGather(copies, g1, gg, z, zs, by_units),
    ]
    ring = RingSum(copies, parts, relay, arrived, y, *ys, 96)
    for job in early + late:
        job.start()
    turned = (((0,), (0,)), ((), ()))
    for n in range(2):
        part = lax.dot_general(
            mixed[n, 0:128], out_small[...], turned, preferred_element_type=jnp.float32
        ) + lax.dot_general(mixed[n, 128:256], out_large[...], turned, preferred_element_type=jnp.float32)
        terms[2 * n : 2 * n + 2] = part.astype(jnp.bfloat16).reshape(2, 2, *residual.shape)
    total = pair_sum(copies, terms, other, ring, y, core, mate)
    for job in early:
        job.pass_on()
    attended = ring.finish(total).astype(jnp.bfloat16).astype(jnp.float32)
    value = residual[...].astype(jnp.float32) + attended
    stream[...] = value
    scale = lax.rsqrt(jnp.mean(value * value, axis=-1, keepdims=True) + 1e-06)
    own[...] = (value * scale * gain[...].astype(jnp.float32)).astype(jnp.bfloat16)

    right, left = ys
    before, after, far = (y + 3) % 4, (y + 1) % 4, (y + 2) % 4
    top, low = pl.ds(0, 48), pl.ds(48, 48)
    sent = (
        copies.make(own.at[top], whole.at[y, core, top], right),
        copies.make(own.at[low], whole.at[y, core, low], left),
        copies.make(own.at[low], whole.at[y, core, low], right),
        copies.make(own.at[top], whole.at[y, core, top], left),
        copies.make(own, whole.at[y, core], mate),
    )
    for copy in sent:
        copy.start()
    whole[y, core] = own[...]
    over = [sent[4]]

    def send(block, device):
        copy = copies.make(block, block, device)
        copy.start()
        return copy

    sent[0].wait_recv()
    on_right = send(whole.at[before, core, top], right)
    over.append(send(whole.at[before, core, top], mate))
    sent[1].wait_recv()
    on_left = send(whole.at[after, core, low], left)
    over.append(send(whole.at[after, core, low], mate))
    for job in late:
        job.pass_on()
    sent[2].wait_recv()
    over.append(send(whole.at[before, core, low], mate))
    sent[3].wait_recv()
    over.append(send(whole.at[after, core, top], mate))
    on_right.wait_recv()
    over.append(send(whole.at[far, core, top], mate))
    on_left.wait_recv()
    over.append(send(whole.at[far, core, low], mate))
    for copy in over:
        copy.wait_recv()
    for job in early + late:
        job.finish()
    copies.drain_sends()


HEADS = ((0, 0, 0, 64), (1, 0, 64, 64), (2, 128, 128, 128))


def selector(head):
    rows = lax.broadcasted_iota(jnp.int32, (128, TILE), 0)
    pieces, rest = [], LOG2E
    for _ in range(3):
        piece = float(np.asarray(rest, dtype=jnp.bfloat16.dtype).astype(np.float64))
        pieces.append(piece)
        rest -= piece
    value = jnp.zeros((128, TILE), jnp.float32)
    for n, piece in enumerate(pieces):
        value = jnp.where(rows == 3 * head + n, piece, value)
    return value.astype(jnp.bfloat16)


def attend_kernel(
    qa_ref, qb_ref, k_ref, off_ref, spread_ref, v_ref, o_ref, tot_ref, work_ref, rhs_ref, ext_ref,
    wide_ref,
):
    z, x = sp_coords()
    kb = pl.program_id(0)

    wide_ref[...] = lax.dot_general(
        off_ref[0], spread_ref[...], (((0,), (0,)), ((), ())), preferred_element_type=jnp.float32
    )
    for j in range(0, STRIPE, 2):
        pair = [eight_keys(wide_ref, j), eight_keys(wide_ref, j + 1)]
        ext_ref[j * 8 : j * 8 + 16, :] = jnp.concatenate(pair, axis=0).astype(jnp.bfloat16)

    @pl.when(kb == 0)
    def _():
        tot_ref[...] = jnp.zeros_like(tot_ref)
        for head, key_column, row, rows in HEADS:
            rhs_ref[head, 128:256, :] = selector(head)
            if rows == 64:
                rhs_ref[head, 64 - row : 128 - row, :] = jnp.zeros((64, TILE), jnp.bfloat16)

    def tile(i, q_ref, group, own_z):
        first = pl.multiple_of(i * TILE, TILE)
        columns = pl.ds(pl.multiple_of(group * 2 * BLOCK + i * TILE, TILE), TILE)

        def run(masked):
            for head, key_column, row, rows in HEADS:
                inner = row if rows == 64 else 0
                for n in range(2):
                    piece = 2 * i + n
                    rhs_ref[head, inner : inner + rows, n * 128 : (n + 1) * 128] = q_ref[
                        piece // 3, row : row + rows, pl.ds(pl.multiple_of(piece % 3 * 128, 128), 128)
                    ]
                rhs = rhs_ref[head]
                sums = jnp.zeros((8, TILE), jnp.float32)
                chunk = 128
                if masked:
                    query = lax.broadcasted_iota(jnp.int32, (1, TILE), 1) + first
                    query_pos = query + (query // HALF - x * 2 + group) * HALF
                for c in reversed(range(BLOCK // chunk)):
                    span = slice(c * chunk, (c + 1) * chunk)
                    lhs = jnp.concatenate(
                        [k_ref[0, span, key_column : key_column + 128], ext_ref[span, :]], axis=1
                    )
                    logit = jnp.dot(lhs, rhs, preferred_element_type=jnp.float32)
                    loss = jnp.maximum(
                        logit, jnp.log2(1.0 + jnp.exp2(jnp.minimum(logit, 100.0)))
                    )
                    if masked:
                        at = lax.broadcasted_iota(jnp.int32, (chunk, TILE), 0) + c * chunk
                        key_pos = (at % 8) * STRIPE + at // 8
                        live = key_pos < query_pos
                        loss = jnp.where(live, loss, 0.0)
                        logit = jnp.where(live, logit, -1e30)
                    for j in reversed(range(chunk // 8)):
                        eight = slice(j * 8, (j + 1) * 8)
                        sums = sums + loss[eight]
                        work_ref[c * chunk + j * 8 : c * chunk + (j + 1) * 8, :] = logit[eight] - sums
                later = [jnp.zeros((1, TILE), jnp.float32)]
                for r in range(7, 0, -1):
                    later.append(later[-1] + sums[r : r + 1])
                tot_ref[pl.ds(kb * 4 + head, 1), columns] = later[-1] + sums[0:1]
                behind = jnp.concatenate(later[::-1], axis=0)
                total = jnp.zeros((rows, TILE), jnp.float32)
                for c in range(BLOCK // 256):
                    span = slice(c * 256, (c + 1) * 256)
                    power = work_ref[span, :].reshape(32, 8, TILE) - behind[None]
                    weight = jnp.exp2(power).reshape(256, TILE).astype(jnp.bfloat16)
                    total = total + jnp.dot(
                        v_ref[0, row : row + rows, span], weight, preferred_element_type=jnp.float32
                    )
                o_ref[0, row : row + rows, columns] = total.astype(jnp.bfloat16)

        place, last = first // HALF, (first + TILE - 1) // HALF
        whole = jnp.logical_or(kb < own_z, jnp.logical_and(kb == own_z, place > x))
        none = jnp.logical_or(kb > own_z, jnp.logical_and(kb == own_z, last < x))
        partly = jnp.logical_not(jnp.logical_or(whole, none))

        @pl.when(whole)
        def _():
            run(False)

        @pl.when(partly)
        def _():
            run(True)

        @pl.when(none)
        def _():
            o_ref[0, :, columns] = jnp.zeros((256, TILE), jnp.bfloat16)

    for group, q_ref in enumerate((qa_ref, qb_ref)):

        def body(i, carry, group=group, q_ref=q_ref):
            tile(i, q_ref, group, z if group == 0 else 3 - z)
            return carry

        lax.fori_loop(0, 6, body, 0)


def attend(qa, qb, k_all, off_all, spread, v_all):
    return pl.pallas_call(
        attend_kernel,
        grid=(4,),
        in_specs=[
            pl.BlockSpec((4, 256, HALF), lambda kb: (0, 0, 0)),
            pl.BlockSpec((4, 256, HALF), lambda kb: (0, 0, 0)),
            pl.BlockSpec((1, BLOCK, 256), lambda kb: (kb, 0, 0)),
            pl.BlockSpec((1, 32, BLOCK), lambda kb: (kb, 0, 0)),
            pl.BlockSpec((32, 128), lambda kb: (0, 0)),
            pl.BlockSpec((1, 256, BLOCK), lambda kb: (kb, 0, 0)),
        ],
        out_specs=[
            pl.BlockSpec((1, 256, 4 * BLOCK), lambda kb: (kb, 0, 0)),
            pl.BlockSpec((16, 4 * BLOCK), lambda kb: (0, 0)),
        ],
        out_shape=[
            jax.ShapeDtypeStruct((4, 256, 4 * BLOCK), jnp.bfloat16),
            jax.ShapeDtypeStruct((16, 4 * BLOCK), jnp.float32),
        ],
        scratch_shapes=[
            pltpu.VMEM((BLOCK, TILE), jnp.float32),
            pltpu.VMEM((3, 256, TILE), jnp.bfloat16),
            pltpu.VMEM((BLOCK, 128), jnp.bfloat16),
            pltpu.VMEM((BLOCK, 128), jnp.float32),
        ],
        compiler_params=pltpu.CompilerParams(
            dimension_semantics=("arbitrary",), vmem_limit_bytes=VMEM_LIMIT
        ),
        cost_estimate=pl.CostEstimate(
            flops=100_000_000_000, bytes_accessed=12_000_000, transcendentals=130_000_000
        ),
        name="attend",
    )(qa, qb, k_all, off_all, spread, v_all)


def sum_scratch(shape):
    bf16 = jnp.bfloat16
    return [
        pltpu.VMEM((4, *shape), bf16),
        pltpu.VMEM((4, *shape), bf16),
        pltpu.VMEM((2, shape[0] // 2, shape[1]), bf16),
        pltpu.VMEM((2, *shape), bf16),
    ]


def feed_kernel(
    rows, g1, gg, u1, uu, d1, dd1, d2, dd2, out, r_vmem, gate_w, up_w, down_w, gate, hidden, terms, other, parts,
    relay, arrived, sems, send_sems, recv_sems,
):
    z, x = sp_coords()
    y, core = tp_place()
    ys, mate = y_neighbours(), sibling()
    greet((*ys, mate))
    copies = Copies(send_sems, recv_sems)
    ring = RingSum(copies, parts, relay, arrived, y, *ys, 96)
    half = d1.shape[1]
    row_copy = pltpu.make_async_copy(rows, r_vmem, sems.at[64])
    row_copy.start()
    waits = [[], [], []]

    def fetch(stage, mine, own, other, dst, n):
        kept = pltpu.make_async_copy(own, dst, sems.at[n])
        came = pltpu.make_async_copy(other, dst, sems.at[n])
        pl.when(mine)(kept.start)
        pl.when(jnp.logical_not(mine))(came.start)
        waits[stage].append(came)

    spots = [(zp, xp, pl.ds((zp * 4 + xp) * 128, 128)) for zp in range(4) for xp in range(4)]
    for n, (zp, xp, lanes) in enumerate(spots):
        fetch(0, z == zp, g1.at[xp], gg.at[zp, xp], gate_w.at[:, lanes], n)
    for n, (zp, xp, lanes) in enumerate(spots):
        fetch(1, x == xp, u1.at[zp], uu.at[xp, zp], up_w.at[:, lanes], 16 + n)
    for n, (zp, xp, lanes) in enumerate(spots):
        fetch(2, z == zp, d1.at[xp], dd1.at[zp, xp], down_w.at[pl.ds(0, half), lanes], 32 + n)
        fetch(2, x == xp, d2.at[zp], dd2.at[xp, zp], down_w.at[pl.ds(half, half), lanes], 48 + n)
    turned = (((1,), (1,)), ((), ()))

    def over_rows(step):
        lax.fori_loop(0, 3, lambda i, c: (step(pl.ds(pl.multiple_of(i * 256, 256), 256)), c)[1], 0)

    row_copy.wait()
    for copy in waits[0]:
        copy.wait()

    def gates(span):
        gate[span, :] = lax.dot_general(
            r_vmem[span, :], gate_w[...], turned, preferred_element_type=jnp.float32
        )

    over_rows(gates)
    for copy in waits[1]:
        copy.wait()

    def hide(span):
        upper = lax.dot_general(
            r_vmem[span, :], up_w[...], turned, preferred_element_type=jnp.float32
        )
        value = gate[span, :]
        hidden[span, :] = (value / (1.0 + jnp.exp(-value)) * upper).astype(jnp.bfloat16)

    over_rows(hide)
    for copy in waits[2]:
        copy.wait()

    order = (ring.far, ring.after, ring.before, y)
    sends = (ring.send_far, ring.send_after, ring.send_before)
    given = []

    def add(n):
        given[n].wait_recv()
        parts[order[n]] = plus(terms[order[n], core], other[order[n]])
        sends[n]()

    for n, place in enumerate(order):
        span = pl.ds(pl.multiple_of(place * 192, 64), 192)
        down = jnp.dot(hidden[span, :], down_w[...], preferred_element_type=jnp.float32)
        terms[place] = down.astype(jnp.bfloat16).reshape(2, 96, 2048)
        copy = copies.make(terms.at[place, 1 - core], other.at[place], mate)
        copy.start()
        given.append(copy)
        if n:
            add(n - 1)
    ring.pass_on()
    given[3].wait_recv()
    own = terms[y, core].astype(jnp.float32) + other[y].astype(jnp.float32)
    out[...] = ring.finish(own).astype(jnp.bfloat16)
    copies.drain_sends()


def feed(rows, *weights):
    units = weights[0].shape[1]
    bf16 = jnp.bfloat16
    shape = (96, 2048)
    return comm_call(
        feed_kernel,
        [(shape, bf16, vmem())],
        [
            pltpu.VMEM((BLOCK, 2048), bf16),
            pltpu.VMEM((units, 2048), bf16),
            pltpu.VMEM((units, 2048), bf16),
            pltpu.VMEM((units, 2048), bf16),
            pltpu.VMEM((BLOCK, units), jnp.float32),
            pltpu.VMEM((BLOCK, units), bf16),
            pltpu.VMEM((4, 2, *shape), bf16),
            *sum_scratch(shape),
            pltpu.SemaphoreType.DMA((65,)),
        ],
        10,
        5,
        "feed",
        [(array, hbm()) for array in (rows, *weights)],
    )[0]


def eight_keys(ref, j):
    return ref[pl.ds(j, STRIPES, stride=STRIPE), :]


def prepare_kernel(qs, ks, vs, ql, kl, vl, q_own, q_give, key, value, wide, turned):
    f32, bf16 = jnp.float32, jnp.bfloat16
    for n, (q, depth) in enumerate(((qs, SMALL_DIM), (ql, LARGE_DIM))):
        rows = slice(n * 128, (n + 1) * 128)
        flipped = (q[...].astype(f32) * float(np.float32(LOG2E * depth**-0.5))).T.astype(bf16)
        q_own[rows, :] = flipped[:, :HALF]
        q_give[rows, :] = flipped[:, HALF:]
    for n, (k, v) in enumerate(((ks, vs), (kl, vl))):
        columns = slice(n * 128, (n + 1) * 128)
        wide[2 * n] = k[...].astype(f32)
        wide[2 * n + 1] = v[...].astype(f32)
        for j in range(0, STRIPE, 2):
            pair = [eight_keys(wide.at[2 * n], j), eight_keys(wide.at[2 * n], j + 1)]
            key[j * 8 : j * 8 + 16, columns] = jnp.concatenate(pair, axis=0).astype(bf16)
            for i in (j, j + 1):
                turned[n, i * 8 : i * 8 + 8, :] = eight_keys(wide.at[2 * n + 1], i)
        value[columns, :] = turned[n].T.astype(bf16)


def prepare(*arrays):
    bf16 = jnp.bfloat16
    shapes = ((256, HALF), (256, HALF), (BLOCK, 256), (256, BLOCK))
    return pl.pallas_call(
        prepare_kernel,
        out_shape=[jax.ShapeDtypeStruct(shape, bf16) for shape in shapes],
        in_specs=[vmem()] * 6,
        out_specs=[vmem()] * 4,
        scratch_shapes=[
            pltpu.VMEM((4, BLOCK, 128), jnp.float32),
            pltpu.VMEM((2, BLOCK, 128), jnp.float32),
        ],
        name="prepare",
    )(*arrays)


def on_device(
    query_small, key_small, value_small, offset_small, query_large, key_large, value_large, offset_large,
    out_small, out_large, residual, norm_gain, gate_weight, up_weight, down_weight,
):
    f32, bf16 = jnp.float32, jnp.bfloat16
    q_own, q_give, key, value = prepare(
        query_small, key_small, value_small, query_large, key_large, value_large
    )
    offsets = jnp.concatenate([offset_small, offset_large], axis=0)
    offsets = jnp.pad(offsets, ((0, 29), (0, 0)))
    gate, up, down = gate_weight.T, up_weight.T, down_weight
    units = down.shape[0]
    qa_all, qb_all, k_all, v_all, off_all, g1, d1 = comm_call(
        gather_kernel,
        [
            ((4, 256, HALF), bf16, vmem()),
            ((4, 256, HALF), bf16, vmem()),
            ((4, BLOCK, 256), bf16, vmem()),
            ((4, 256, BLOCK), bf16, vmem()),
            ((4, 32, BLOCK), bf16, vmem()),
            ((4, units, 128), bf16, hbm()),
            ((4, units // 2, 128), bf16, hbm()),
        ],
        [pltpu.VMEM((256, HALF), bf16), pltpu.SemaphoreType.DMA((2,))],
        43,
        0,
        "gather_qkv",
        [(array, vmem()) for array in (q_own, q_give, key, value, offsets, gate, down)],
    )
    spread = np.zeros((32, 128), np.float32)
    for head in range(3):
        spread[head, 3 * head : 3 * head + 3] = 1
    outs, totals = attend(qa_all, qb_all, k_all, off_all, jnp.asarray(spread, bf16), v_all)
    half = (256, HALF)
    buffers = [pltpu.VMEM((4, 16, 4 * BLOCK), f32), pltpu.VMEM((4, 256, 4 * BLOCK), bf16)]
    for shape in ((4, *half), (2, 128, HALF), (2, *half), half):
        buffers += [pltpu.VMEM(shape, bf16)] * 2
    mixed, u1, d2 = comm_call(
        mix_kernel,
        [
            ((2, *half), bf16, vmem()),
            ((4, units, 128), bf16, hbm()),
            ((4, units // 2, 128), bf16, hbm()),
        ],
        [*buffers, pltpu.SemaphoreType.DMA((2,)), pltpu.SemaphoreType.DMA((8,))],
        31,
        1,
        "mix",
        [(totals, vmem()), (up, vmem()), (down, vmem()), (outs, hbm())],
    )
    shape = residual.shape
    stream, rows, dd1, dd2, gg, uu = comm_call(
        middle_kernel,
        [
            (shape, f32, vmem()),
            ((4, 2, *shape), bf16, vmem()),
            ((4, *d1.shape), bf16, hbm()),
            ((4, *d2.shape), bf16, hbm()),
            ((4, *g1.shape), bf16, hbm()),
            ((4, *u1.shape), bf16, hbm()),
        ],
        [*sum_scratch(shape), pltpu.VMEM(shape, bf16), pltpu.VMEM((4, 2, *shape), bf16)],
        47,
        3,
        "middle",
        [
            (array, vmem())
            for array in (mixed, out_small, out_large, residual, norm_gain.astype(f32).reshape(1, -1))
        ]
        + [(array, hbm()) for array in (d1, d2, g1, u1)],
    )
    summed = feed(rows.reshape(BLOCK, 2048), g1, gg, u1, uu, d1, dd1, d2, dd2)
    return (stream + summed.astype(f32)).astype(bf16)


def solution(mesh):
    return jax.shard_map(
        on_device,
        mesh=mesh,
        in_specs=(
            P("sp", "tp"), P("sp", "tp"), P("sp", "tp"), P("tp", "sp"),
            P("sp", "tp"), P("sp", "tp"), P("sp", "tp"), P("tp", "sp"),
            P("tp", None), P("tp", None), P(("sp", "tp"), None), P(),
            P("sp", "tp"), P("sp", "tp"), P("tp", "sp"),
        ),
        out_specs=P(("sp", "tp"), None),
        check_vma=False,
    )
```
